256 devices in a mesh: ep: 16 (over y, x), tp: 16 (over z, core).
Axes of the slice: x: 4, y: 4, z: 8, core: 2. Of those that a mesh axis runs over, the one named last changes fastest.
Arguments:
- mix_tokens: bfloat16 [4096, 4096], P('ep'), may hold values from -6 to 6
- mix_gain: float32 [4096], replicated, may hold values from 0.1 to 1.9
- value_weight: bfloat16 [4096, 2048], P(None, 'tp'), may hold values from -0.09375 to 0.09375
- inner_weight: bfloat16 [4096, 2048], P(None, 'tp'), may hold values from -0.09375 to 0.09375
- outer_weight: bfloat16 [4096, 2048], P(None, 'tp'), may hold values from -0.09375 to 0.09375
- conv_taps: float32 [3, 2048], P(None, 'tp'), may hold values from -3 to 3
- mix_weight: bfloat16 [2048, 4096], P('tp'), may hold values from -0.125 to 0.125
- moe_tokens: bfloat16 [4096, 4096], P('ep'), may hold values from -6 to 6
- moe_gain: float32 [4096], replicated, may hold values from 0.1 to 1.9
- router_group: bfloat16 [4096, 4], replicated, may hold values from -0.09375 to 0.09375
- router_expert: bfloat16 [4096, 16], replicated, may hold values from -0.09375 to 0.09375
- expert_routes: int32 [4096, 2], P('ep'), may hold values from 0 to 15, as said below
- gate_weight: bfloat16 [16, 4096, 2048], P('ep', None, 'tp'), may hold values from -0.09375 to 0.09375
- up_weight: bfloat16 [16, 4096, 2048], P('ep', None, 'tp'), may hold values from -0.09375 to 0.09375
- down_weight: bfloat16 [16, 2048, 4096], P('ep', 'tp'), may hold values from -0.5 to 0.5
Outputs:
- mixer_out: bfloat16 [4096, 4096], P(('ep', 'tp'))
- expert_out: bfloat16 [4096, 4096], P(('ep', 'tp'))
The draws below stay inside these ranges and needn't reach their ends.
Inputs may be any that keep to these rules, and one draw needn't show every extreme that they name: `expert_routes`: the two experts of a row are different and lie in one group of 4 consecutive expert numbers. In each aligned block of 16 rows no expert is named more than 4 times, and in every draw some experts are named exactly 4 times in every block.
All inputs are finite; a program needn't handle non-finite values.
Results may differ from the reference program's by a relative error of at most 0.0076.
Values may be sent and summed in bfloat16 or wider, within the bound.
A program may use at most 128 MiB of HBM per device.

```python
import jax
import jax.numpy as jnp
from jax import lax

D = 4096
CONV_CH = 2048
TAPS = 3
FE = 2048
EXPERTS = 16
GROUPS = 4
TOPK = 2
MOE_SHARE = 16
EPG = 4
CAP = 4
MIX_TOKENS = 4096
MOE_TOKENS = 4096


def draw_expert_routes(key, part):
    blocks = MOE_TOKENS // MOE_SHARE
    half_share = MOE_SHARE // 2
    subkeys = jax.random.split(jax.random.fold_in(key, 7), 5)
    hot_group = jax.random.randint(subkeys[0], (), 0, GROUPS).astype(jnp.int32)
    others = (hot_group + 1 + jax.random.randint(subkeys[1], (blocks, MOE_SHARE - half_share), 0, GROUPS - 1)) % GROUPS
    labels = jnp.concatenate([jnp.full((blocks, half_share), hot_group, jnp.int32), others.astype(jnp.int32)], axis=1)
    scores = jax.random.randint(subkeys[2], (blocks, MOE_SHARE), 0, 1048576) * MOE_SHARE + jnp.arange(MOE_SHARE, dtype=jnp.int32)[None, :]
    ordering = jnp.argsort(scores, axis=1, stable=True)
    labels = jnp.take_along_axis(labels, ordering, axis=1)
    one_hot = (labels[:, :, None] == jnp.arange(GROUPS, dtype=jnp.int32)[None, None, :]).astype(jnp.int32)
    within = jnp.sum((jnp.cumsum(one_hot, axis=1) - one_hot) * one_hot, axis=2)
    offsets = jax.random.randint(subkeys[3], (blocks, GROUPS), 0, EPG)
    strides = jax.random.randint(subkeys[4], (blocks, GROUPS), 1, EPG)
    offset_tok = jnp.take_along_axis(offsets, labels, axis=1)
    stride_tok = jnp.take_along_axis(strides, labels, axis=1)
    first_pick = labels * EPG + (within + offset_tok) % EPG
    second_pick = labels * EPG + (within + offset_tok + stride_tok) % EPG
    return jnp.stack([first_pick, second_pick], axis=-1).reshape(blocks * MOE_SHARE, TOPK).astype(jnp.int32)


def levels(rng, shape, cuts, smallest, top_value):
    loudness = 1.0
    for dim, shards_of in cuts:
        draws = jax.random.uniform(jax.random.fold_in(jax.random.fold_in(rng, 6), dim), (shards_of,), jnp.float32, smallest / len(cuts), top_value / len(cuts))
        loudness = loudness * jnp.repeat(jnp.exp(draws), shape[dim] // shards_of).reshape((-1,) + (1,) * (len(shape) - 1 - dim))
    return loudness


def bell_draw(own_key, dims, deviation, limit, cuts=(), kind=jnp.bfloat16):
    values = deviation * jax.random.normal(own_key, dims, jnp.float32)
    if cuts:
        values = values * levels(own_key, dims, cuts, -0.22, 0.18)
    return jnp.clip(values, -limit, limit).astype(kind)


def setup_inputs(seed: int = 0) -> dict:
    seeds = jax.random.split(jax.random.key(seed), 16)
    return {
        "mix_tokens": bell_draw(seeds[0], (MIX_TOKENS, D), 1.0, 6.0, ((0, 16),)),
        "mix_gain": jnp.clip(1.0 + 0.18 * jax.random.normal(seeds[1], (D,), jnp.float32), 0.1, 1.9),
        "value_weight": bell_draw(seeds[2], (D, CONV_CH), D ** -0.5, 0.09375, ((1, 16),)),
        "inner_weight": bell_draw(seeds[3], (D, CONV_CH), D ** -0.5, 0.09375, ((1, 16),)),
        "outer_weight": bell_draw(seeds[4], (D, CONV_CH), D ** -0.5, 0.09375, ((1, 16),)),
        "conv_taps": bell_draw(seeds[5], (TAPS, CONV_CH), 0.6, 3.0, ((1, 16),), jnp.float32),
        "mix_weight": bell_draw(seeds[6], (CONV_CH, D), CONV_CH ** -0.5, 0.125, ((0, 16),)),
        "moe_tokens": bell_draw(seeds[7], (MOE_TOKENS, D), 1.0, 6.0, ((0, 16),)),
        "moe_gain": jnp.clip(1.0 + 0.18 * jax.random.normal(seeds[8], (D,), jnp.float32), 0.1, 1.9),
        "router_group": bell_draw(seeds[9], (D, GROUPS), D ** -0.5, 0.09375),
        "router_expert": bell_draw(seeds[10], (D, EXPERTS), D ** -0.5, 0.09375),
        "expert_routes": draw_expert_routes(jax.random.fold_in(seeds[15], 71), 0),
        "gate_weight": bell_draw(seeds[12], (EXPERTS, D, FE), D ** -0.5, 0.09375, ((0, 16), (2, 16))),
        "up_weight": bell_draw(seeds[13], (EXPERTS, D, FE), D ** -0.5, 0.09375, ((0, 16), (2, 16))),
        "down_weight": bell_draw(seeds[14], (EXPERTS, FE, D), (FE // 16) ** -0.5, 0.5, ((0, 16), (1, 16))),
    }


def rms_rows(inputs, gain_vec):
    values = inputs.astype(jnp.float32)
    inverse = lax.rsqrt(lax.optimization_barrier(jnp.mean(values * values, axis=-1, keepdims=True)) + 1e-06)
    return (values * inverse * gain_vec.astype(jnp.float32)).astype(jnp.bfloat16)

def route_weights(normed, routes, router_group, router_expert):
    group_logit = jnp.dot(normed, router_group, preferred_element_type=jnp.float32)
    expert_logit = jnp.dot(normed, router_expert, preferred_element_type=jnp.float32)
    group_exp = jnp.exp(group_logit)
    group_id = routes[:, 0] // EPG
    group_pick = (group_id[:, None] == jnp.arange(GROUPS, dtype=jnp.int32)[None, :]).astype(jnp.float32)
    group_gate = lax.optimization_barrier(jnp.sum(group_exp * group_pick, axis=1)) / lax.optimization_barrier(jnp.sum(group_exp, axis=1))
    expert_pick = (routes[:, :, None] == jnp.arange(EXPERTS, dtype=jnp.int32)[None, None, :]).astype(jnp.float32)
    chosen = jnp.exp(lax.optimization_barrier(jnp.sum(expert_logit[:, None, :] * expert_pick, axis=2)))
    return group_gate[:, None] * chosen / lax.optimization_barrier(jnp.sum(chosen, axis=1, keepdims=True))

def slot_ranks(routes):
    blocks = routes.shape[0] // MOE_SHARE
    entries = routes.reshape(blocks, MOE_SHARE * TOPK)
    one_hot = (entries[:, :, None] == jnp.arange(EXPERTS, dtype=jnp.int32)[None, None, :]).astype(jnp.int32)
    before = jnp.cumsum(one_hot, axis=1) - one_hot
    return lax.optimization_barrier(jnp.sum(before * one_hot, axis=2)).reshape(routes.shape)

def reference(mix_tokens, mix_gain, value_weight, inner_weight, outer_weight, conv_taps, mix_weight, moe_tokens, moe_gain, router_group, router_expert, expert_routes, gate_weight, up_weight, down_weight):
    normed = rms_rows(mix_tokens, mix_gain)
    value_proj = jnp.dot(normed, value_weight, preferred_element_type=jnp.float32)
    inner_proj = jnp.dot(normed, inner_weight, preferred_element_type=jnp.float32)
    outer_proj = jnp.dot(normed, outer_weight, preferred_element_type=jnp.float32)
    gated_in = lax.optimization_barrier((inner_proj * value_proj).astype(jnp.bfloat16)).astype(jnp.float32)
    seq_rows = gated_in.shape[0]
    padded = jnp.concatenate([jnp.zeros((TAPS - 1, gated_in.shape[1]), jnp.float32), gated_in], axis=0)
    tap_values = conv_taps.astype(jnp.float32)
    mixed_conv = tap_values[0] * padded[0:seq_rows]
    for tap_index in range(1, TAPS):
        mixed_conv = mixed_conv + tap_values[tap_index] * padded[tap_index:tap_index + seq_rows]
    conv_out = (outer_proj * mixed_conv).astype(jnp.bfloat16)
    mixer_out = jnp.dot(conv_out, mix_weight, preferred_element_type=jnp.float32).astype(jnp.bfloat16)
    moe_normed = rms_rows(moe_tokens, moe_gain)
    weights = route_weights(moe_normed, expert_routes, router_group, router_expert)
    ranks = slot_ranks(expert_routes)
    total_rows = moe_tokens.shape[0]
    block_id = jnp.arange(total_rows, dtype=jnp.int32) // MOE_SHARE
    position = (block_id[:, None] * CAP + ranks).astype(jnp.int32)
    per_expert = total_rows // MOE_SHARE * CAP
    token_id = jnp.broadcast_to(jnp.arange(total_rows, dtype=jnp.int32)[:, None], (total_rows, TOPK))
    slot_table = jnp.zeros((EXPERTS, per_expert), jnp.int32).at[expert_routes, position].set(token_id)

    def run_expert(operands):
        row_index, gate_w, up_w, down_w = operands
        picked_rows = moe_normed[row_index]
        gate_proj = jnp.dot(picked_rows, gate_w, preferred_element_type=jnp.float32)
        up_proj = jnp.dot(picked_rows, up_w, preferred_element_type=jnp.float32)
        hidden = (jax.nn.silu(gate_proj) * up_proj).astype(jnp.bfloat16)
        summed = jnp.dot(hidden, down_w, preferred_element_type=jnp.float32)
        return summed.astype(jnp.bfloat16)
    results = lax.map(run_expert, (slot_table, gate_weight, up_weight, down_weight))
    picked = results[expert_routes, position].astype(jnp.float32)
    expert_out = lax.optimization_barrier(jnp.sum(weights[:, :, None] * picked, axis=1)).astype(jnp.bfloat16)
    return (mixer_out, expert_out)
```

```python
import functools

import jax
import jax.numpy as jnp
from jax import lax
from jax.experimental import pallas as pl
from jax.experimental.pallas import tpu as pltpu
from jax.sharding import PartitionSpec as P

MESH = pl.DeviceIdType.MESH
F32 = jnp.float32
BF16 = jnp.bfloat16
SHARE = 16
CAP = 4
EPG = 4
EPS = 1e-06
PIECES = 4


def rms_into(raw, gain_ref, out):
    gain = gain_ref[...]

    def body(i, carry):
        rows = pl.ds(pl.multiple_of(i * SHARE, SHARE), SHARE)
        values = raw[rows, :].astype(F32)
        inverse = lax.rsqrt(jnp.mean(values * values, axis=-1, keepdims=True) + EPS)
        out[rows, :] = (values * inverse * gain).astype(BF16)
        return carry

    lax.fori_loop(0, raw.shape[0] // SHARE, body, 0)


def kernel(
    EP,
    Z,
    mix_x,
    mix_gain,
    value_w,
    inner_w,
    outer_w,
    taps,
    mix_w,
    moe_x,
    moe_gain,
    router_g,
    router_e,
    routes,
    gate_w,
    up_w,
    down_w,
    mix_out,
    moe_out,
    raw_m,
    raw_e,
    norm_m,
    norm_e,
    gu_w,
    dn_w,
    proj_w,
    mixw,
    select,
    select_all,
    send,
    recv,
    acc,
    rs_send,
    rs_recv,
    halo_out,
    halo_in,
    gated,
    outer_p,
    conv,
    conv_all,
    mix_part,
    comb_w,
    ret_send,
    ret_recv,
    comb,
    comb_in,
    load_sem,
    swap_send,
    swap_recv,
    disp_send,
    disp_recv,
    hop_send,
    hop_recv,
    halo_sem,
    conv_sem,
    back_send,
    back_recv,
    last_send,
    last_recv,
):
    tokens, width = raw_m.shape
    C = value_w.shape[1]
    F = gate_w.shape[1]
    half = EP // 2
    rows = half * 2 * CAP
    piece = width // PIECES
    hops = Z // 2

    e = lax.axis_index("ep")
    tp = lax.axis_index("tp")
    z, c = tp // 2, lax.rem(tp, 2)
    ep_odd = lax.rem(e, 2)
    slot = e // 2
    partner = (e, z * 2 + 1 - c)

    def to_expert(i):
        return (2 * i + c, z * 2 + 1 - ep_odd)

    def to_source(i):
        return (2 * i + 1 - c, z * 2 + ep_odd)

    def beside(step):
        return (e, lax.rem(z + step + Z, Z) * 2 + c)

    def remote(src, dst, ssem, rsem, device):
        return pltpu.make_async_remote_copy(
            src_ref=src, dst_ref=dst, send_sem=ssem, recv_sem=rsem, device_id=device, device_id_type=MESH
        )

    loads = [
        pltpu.make_async_copy(src, dst, load_sem.at[n])
        for n, (src, dst) in enumerate(
            [
                (moe_x, raw_e),
                (mix_x, raw_m),
                (value_w, proj_w.at[:, 0:C]),
                (inner_w, proj_w.at[:, C : 2 * C]),
                (outer_w, proj_w.at[:, 2 * C : 3 * C]),
                (mix_w, mixw.at[0:C]),
                (gate_w, gu_w.at[:, 0:F]),
                (up_w, gu_w.at[:, 2 * F : 3 * F]),
                (down_w, dn_w.at[0:F]),
            ]
        )
    ]
    for copy in loads:
        copy.start()

    barrier = pltpu.get_barrier_semaphore()
    greet = [to_expert(i) for i in range(half)] + [to_source(i) for i in range(half)]
    greet += [beside(1), beside(-1)]
    greet += [(lax.rem(e + 1, EP), tp), (lax.rem(e + EP - 1, EP), tp)]
    for device in greet:
        pl.semaphore_signal(barrier, inc=1, device_id=device, device_id_type=MESH)

    r0 = routes[0:1, :]
    r1 = routes[1:2, :]
    row = lax.broadcasted_iota(jnp.int32, (rows, tokens), 0)
    tok = lax.broadcasted_iota(jnp.int32, (rows, tokens), 1)
    expert_of = 2 * (row >> 3) + c
    named = (r0 == expert_of) | (r1 == expert_of)
    before_r = lax.broadcasted_iota(jnp.int32, (tokens, tokens), 0)
    before_c = lax.broadcasted_iota(jnp.int32, (tokens, tokens), 1)
    before = ((before_r < before_c) & ((before_r >> 4) == (before_c >> 4))).astype(F32).astype(BF16)
    rank = jnp.dot(named.astype(F32).astype(BF16), before, preferred_element_type=F32)
    hit = named & (rank == (row & 3).astype(F32)) & (((tok >> 4) & 1) == ((row >> 2) & 1))
    hit = hit.astype(F32)
    select[...] = hit

    def home_of(s):
        k = (s + 1) // 2
        sign = 2 * lax.rem(s, 2) - 1
        return lax.rem(z + jnp.where(s == 0, hops, sign * (hops - k)) + Z, Z)

    def stage_select(s):
        t = lax.broadcasted_iota(jnp.int32, (rows, tokens), 1)
        return jnp.where((t >> 5) == home_of(s), select[...], 0.0).astype(BF16)

    loads[0].wait()
    rms_into(raw_e, moe_gain, norm_e)
    first = stage_select(jnp.int32(0))

    def place_first(n, carry):
        cols = pl.ds(pl.multiple_of(n * 512, 512), 512)
        placed = jnp.dot(first, norm_e[:, cols], preferred_element_type=F32)
        send[0, :, :, cols] = placed.reshape(half, 2 * CAP, 512).astype(BF16)
        return carry

    lax.fori_loop(0, width // 512, place_first, 0)

    pl.semaphore_wait(barrier, len(greet))

    def dispatch(s):
        for i in range(half):
            remote(send.at[s, i], recv.at[s, slot], disp_send.at[s], disp_recv.at[s], to_expert(i)).start()

    dispatch(0)
    swaps = [
        remote(src, dst, swap_send.at[n], swap_recv.at[n], partner)
        for n, (src, dst) in enumerate(
            [
                (gate_w, gu_w.at[:, F : 2 * F]),
                (up_w, gu_w.at[:, 3 * F : 4 * F]),
                (mix_w, mixw.at[C : 2 * C]),
                (down_w, dn_w.at[F : 2 * F]),
            ]
        )
    ]
    for copy in swaps:
        copy.start()

    for s in range(1, Z):
        select_all[(s - 1) * rows : s * rows, :] = stage_select(jnp.int32(s))

    def place_rest(n, carry):
        cols = pl.ds(pl.multiple_of(n * 256, 256), 256)
        placed = jnp.dot(select_all[...], norm_e[:, cols], preferred_element_type=F32)
        send[pl.ds(1, Z - 1), :, :, cols] = placed.reshape(Z - 1, half, 2 * CAP, 256).astype(BF16)
        return carry

    lax.fori_loop(0, width // 256, place_rest, 0)

    def dispatch_rest(s, carry):
        dispatch(s)
        return carry

    lax.fori_loop(1, Z, dispatch_rest, 0)

    loads[1].wait()
    rms_into(raw_m, mix_gain, norm_m)
    for n in (2, 3, 4):
        loads[n].wait()
    proj = jnp.dot(norm_m[...], proj_w[...], preferred_element_type=F32)
    gated_in = (proj[:, C : 2 * C] * proj[:, 0:C]).astype(BF16)
    outer_p[...] = proj[:, 2 * C : 3 * C]
    gated[pl.ds(SHARE, tokens), :] = gated_in.astype(F32)
    halo_out[...] = gated_in[tokens - SHARE :, :]
    halo = remote(halo_out, halo_in, halo_sem.at[0], halo_sem.at[1], (lax.rem(e + 1, EP), tp))
    halo.start()

    home = 2 * SHARE
    pick_r = lax.broadcasted_iota(jnp.int32, (tokens, home), 0)
    pick_c = lax.broadcasted_iota(jnp.int32, (tokens, home), 1)
    pick = (pick_r == pick_c + z * home).astype(F32).astype(BF16)
    own = jnp.dot(routes[...].astype(F32).astype(BF16), pick, preferred_element_type=F32)
    h0, h1 = own[0:1, :], own[1:2, :]
    own_normed = norm_e[pl.ds(pl.multiple_of(z * home, home), home), :]
    contract_last = (((1,), (1,)), ((), ()))
    group_logit = lax.dot_general(router_g[...], own_normed, contract_last, preferred_element_type=F32)
    expert_logit = lax.dot_general(router_e[...], own_normed, contract_last, preferred_element_type=F32)
    group_exp = jnp.exp(group_logit)
    first_of = (lax.broadcasted_iota(jnp.int32, group_exp.shape, 0) * EPG).astype(F32)
    in_group = (h0 >= first_of) & (h0 < first_of + EPG)
    gate = jnp.sum(jnp.where(in_group, group_exp, 0.0), axis=0, keepdims=True) / jnp.sum(
        group_exp, axis=0, keepdims=True
    )
    number = lax.broadcasted_iota(jnp.int32, expert_logit.shape, 0).astype(F32)
    chosen0 = jnp.exp(jnp.sum(jnp.where(number == h0, expert_logit, 0.0), axis=0, keepdims=True))
    chosen1 = jnp.exp(jnp.sum(jnp.where(number == h1, expert_logit, 0.0), axis=0, keepdims=True))
    both = chosen0 + chosen1
    w0, w1 = gate * chosen0 / both, gate * chosen1 / both
    row_h = lax.broadcasted_iota(jnp.int32, (rows, home), 0)
    tok_h = lax.broadcasted_iota(jnp.int32, (rows, home), 1)
    expert_h = (2 * (row_h >> 3) + c).astype(F32)
    is0, is1 = h0 == expert_h, h1 == expert_h
    bef_r = lax.broadcasted_iota(jnp.int32, (home, home), 0)
    bef_c = lax.broadcasted_iota(jnp.int32, (home, home), 1)
    bef = ((bef_r < bef_c) & ((bef_r >> 4) == (bef_c >> 4))).astype(F32).astype(BF16)
    rank_h = jnp.dot((is0 | is1).astype(F32).astype(BF16), bef, preferred_element_type=F32)
    at = (rank_h == (row_h & 3).astype(F32)) & ((tok_h >> 4) == ((row_h >> 2) & 1))
    weight = jnp.where(at & is0, w0, 0.0) + jnp.where(at & is1, w1, 0.0)
    weight = weight.T
    high = weight.astype(BF16)
    comb_w[0:home, :] = high
    comb_w[home : 2 * home, :] = (weight - high.astype(F32)).astype(BF16)

    halo.wait()
    gated[0:SHARE, :] = jnp.where(e > 0, halo_in[...].astype(F32), 0.0)
    mixed = taps[0:1, :] * gated[pl.ds(SHARE - 2, tokens), :]
    mixed = mixed + taps[1:2, :] * gated[pl.ds(SHARE - 1, tokens), :]
    mixed = mixed + taps[2:3, :] * gated[pl.ds(SHARE, tokens), :]
    conv_out = (outer_p[...] * mixed).astype(BF16).reshape(Z, 2, SHARE, C)
    conv[0] = conv_out[:, 0].reshape(Z * SHARE, C)
    conv[1] = conv_out[:, 1].reshape(Z * SHARE, C)
    conv_swap = remote(conv.at[1 - c], conv_all.at[:, C : 2 * C], conv_sem.at[0], conv_sem.at[1], partner)
    conv_swap.start()
    conv_all[:, 0:C] = conv[c]
    loads[5].wait()
    swaps[2].wait_recv()
    conv_swap.wait()

    def down_mix(n, carry):
        cols = pl.ds(pl.multiple_of(n * 512, 512), 512)
        part = jnp.dot(conv_all[...], mixw[:, cols], preferred_element_type=F32)
        mix_part[:, :, cols] = part.reshape(Z, SHARE, 512)
        return carry

    lax.fori_loop(0, width // 512, down_mix, 0)
    for n in (6, 7, 8):
        loads[n].wait()
    for n in (0, 1, 3):
        swaps[n].wait_recv()

    def hop(direction, k, j):
        return remote(
            rs_send.at[direction, k, j],
            rs_recv.at[direction, k, j],
            hop_send.at[direction, k, j],
            hop_recv.at[direction, k, j],
            beside(2 * direction - 1),
        )

    def give_back(j, i):
        return remote(ret_send.at[j, i], ret_recv.at[j, slot], back_send.at[j], back_recv.at[j], to_source(i))

    def stage(s, carry):
        arrived = remote(send.at[s], recv.at[s], disp_send.at[s], disp_recv.at[s], partner)
        arrived.wait_recv()
        x = recv[s].reshape(rows, width)
        gate_up = jnp.dot(x, gu_w[...], preferred_element_type=F32)
        g, u = gate_up[:, 0 : 2 * F], gate_up[:, 2 * F :]
        hidden = (g / (1.0 + jnp.exp(-g)) * u).astype(BF16)
        direction = lax.rem(s, 2)
        k = (s + 1) // 2
        zs = home_of(s)
        for j in range(PIECES):
            cols = slice(j * piece, (j + 1) * piece)
            side = 1 if j < PIECES // 2 else 0
            acc[0:rows, :] = jnp.dot(hidden, dn_w[:, cols], preferred_element_type=F32)
            acc[rows:, :] = mix_part[zs, :, cols]

            @pl.when(s == 0)
            def _():
                rs_send[side, 0, j] = acc[...].astype(BF16)
                hop(side, 0, j).start()

            @pl.when((s > 0) & (s < Z - 1))
            def _():
                @pl.when((k > 1) | (direction == side))
                def _():
                    hop(direction, k - 1, j).wait_recv()
                    acc[...] += rs_recv[direction, k - 1, j].astype(F32)

                rs_send[direction, k, j] = acc[...].astype(BF16)
                hop(direction, k, j).start()

            @pl.when(s == Z - 1)
            def _():
                for way in (1, 0):
                    hop(way, hops - 1, j).wait_recv()
                    acc[...] += rs_recv[way, hops - 1, j].astype(F32)
                ret_send[j] = acc[0:rows, :].astype(BF16).reshape(half, 2 * CAP, piece)
                for i in range(half):
                    give_back(j, i).start()
                mix_out[:, cols] = acc[rows:, :].astype(BF16)

        return carry

    lax.fori_loop(0, Z, stage, 0)

    def last(j):
        return remote(comb.at[j, 1 - c], comb_in.at[j], last_send.at[j], last_recv.at[j], partner)

    for j in range(PIECES):
        remote(ret_send.at[j], ret_recv.at[j], back_send.at[j], back_recv.at[j], partner).wait_recv()
        summed = jnp.dot(comb_w[...], ret_recv[j].reshape(rows, piece), preferred_element_type=F32)
        comb[j] = (summed[0:home] + summed[home:]).reshape(2, SHARE, piece)
        last(j).start()
    for j in range(PIECES):
        last(j).wait_recv()
        moe_out[:, j * piece : (j + 1) * piece] = (comb[j, c] + comb_in[j]).astype(BF16)

    for copy in swaps:
        copy.wait_send()
    for s in range(Z):
        remote(send.at[s], recv.at[s], disp_send.at[s], disp_recv.at[s], partner).wait_send()
    for j in range(PIECES):
        hop(1 if j < PIECES // 2 else 0, 0, j).wait_send()
        for k in range(1, hops):
            for direction in (0, 1):
                hop(direction, k, j).wait_send()
        remote(ret_send.at[j], ret_recv.at[j], back_send.at[j], back_recv.at[j], partner).wait_send()
        last(j).wait_send()


def solution(mesh):
    EP, TP = mesh.shape["ep"], mesh.shape["tp"]
    Z = TP // 2

    def local(
        mix_tokens,
        mix_gain,
        value_weight,
        inner_weight,
        outer_weight,
        conv_taps,
        mix_weight,
        moe_tokens,
        moe_gain,
        router_group,
        router_expert,
        expert_routes,
        gate_weight,
        up_weight,
        down_weight,
    ):
        tokens, D = mix_tokens.shape
        C = value_weight.shape[1]
        F = gate_weight.shape[2]
        half = EP // 2
        rows = half * 2 * CAP
        piece = D // PIECES
        hops = Z // 2
        vmem = pl.BlockSpec(memory_space=pltpu.VMEM)
        hbm = pl.BlockSpec(memory_space=pl.ANY)
        V = pltpu.VMEM
        DMA = pltpu.SemaphoreType.DMA
        out = jax.ShapeDtypeStruct((SHARE, D), BF16)
        return pl.pallas_call(
            functools.partial(kernel, EP, Z),
            out_shape=(out, out),
            in_specs=[hbm, vmem, hbm, hbm, hbm, vmem, hbm, hbm, vmem, vmem, vmem, vmem, hbm, hbm, hbm],
            out_specs=(vmem, vmem),
            scratch_shapes=[
                V((tokens, D), BF16),
                V((tokens, D), BF16),
                V((tokens, D), BF16),
                V((tokens, D), BF16),
                V((D, 4 * F), BF16),
                V((2 * F, D), BF16),
                V((D, 3 * C), BF16),
                V((2 * C, D), BF16),
                V((rows, tokens), F32),
                V(((Z - 1) * rows, tokens), BF16),
                V((Z, half, 2 * CAP, D), BF16),
                V((Z, half, 2 * CAP, D), BF16),
                V((rows + SHARE, piece), F32),
                V((2, hops, PIECES, rows + SHARE, piece), BF16),
                V((2, hops, PIECES, rows + SHARE, piece), BF16),
                V((SHARE, C), BF16),
                V((SHARE, C), BF16),
                V((SHARE + tokens, C), F32),
                V((tokens, C), F32),
                V((2, Z * SHARE, C), BF16),
                V((Z * SHARE, 2 * C), BF16),
                V((Z, SHARE, D), F32),
                V((4 * SHARE, rows), BF16),
                V((PIECES, half, 2 * CAP, piece), BF16),
                V((PIECES, half, 2 * CAP, piece), BF16),
                V((PIECES, 2, SHARE, piece), F32),
                V((PIECES, SHARE, piece), F32),
                DMA((9,)),
                DMA((4,)),
                DMA((4,)),
                DMA((Z,)),
                DMA((Z,)),
                DMA((2, hops, PIECES)),
                DMA((2, hops, PIECES)),
                DMA((2,)),
                DMA((2,)),
                DMA((PIECES,)),
                DMA((PIECES,)),
                DMA((PIECES,)),
                DMA((PIECES,)),
            ],
            compiler_params=pltpu.CompilerParams(
                collective_id=0, has_side_effects=True, vmem_limit_bytes=60 * 1024 * 1024
            ),
            name="mixer_and_experts",
        )(
            mix_tokens,
            mix_gain.reshape(1, D),
            value_weight,
            inner_weight,
            outer_weight,
            conv_taps,
            mix_weight,
            moe_tokens,
            moe_gain.reshape(1, D),
            router_group.T,
            router_expert.T,
            expert_routes.T,
            gate_weight.reshape(D, F),
            up_weight.reshape(D, F),
            down_weight.reshape(F, D),
        )

    return jax.shard_map(
        local,
        mesh=mesh,
        in_specs=(
            P("ep", None),
            P(),
            P(None, "tp"),
            P(None, "tp"),
            P(None, "tp"),
            P(None, "tp"),
            P("tp", None),
            P("ep", None),
            P(),
            P(),
            P(),
            P("ep", None),
            P("ep", None, "tp"),
            P("ep", None, "tp"),
            P("ep", "tp", None),
        ),
        out_specs=(P(("ep", "tp"), None), P(("ep", "tp"), None)),
        check_vma=False,
    )
```

```python
import functools

import jax
import jax.numpy as jnp
from jax import lax
from jax.experimental import pallas as pl
from jax.experimental.pallas import tpu as pltpu
from jax.sharding import PartitionSpec as P

MESH = pl.DeviceIdType.MESH
F32 = jnp.float32
BF16 = jnp.bfloat16
SHARE = 16
CAP = 4
EPG = 4
EPS = 1e-06
PIECES = 4
AHEAD = 3


def rms_rows(raw, gain, out, start, count):
    def body(i, carry):
        rows = pl.ds(pl.multiple_of(start + i * SHARE, SHARE), SHARE)
        values = raw[rows, :].astype(F32)
        inverse = lax.rsqrt(jnp.mean(values * values, axis=-1, keepdims=True) + EPS)
        out[rows, :] = (values * inverse * gain).astype(BF16)
        return carry

    lax.fori_loop(0, count // SHARE, body, 0)


def kernel(
    EP,
    Z,
    mix_x,
    mix_gain,
    value_w,
    inner_w,
    outer_w,
    taps,
    mix_w,
    moe_x,
    moe_gain,
    router_g,
    router_e,
    routes,
    gate_w,
    up_w,
    down_w,
    mix_out,
    moe_out,
    raw_m,
    raw_e,
    norm_m,
    norm_e,
    gu_w,
    dn_w,
    proj_w,
    mixw,
    send,
    recv,
    acc,
    rs_send,
    rs_recv,
    halo_out,
    halo_in,
    gated,
    outer_p,
    conv,
    conv_all,
    mix_part,
    comb_w,
    ret_send,
    ret_recv,
    comb,
    comb_in,
    load_sem,
    tok_sem,
    swap_send,
    swap_recv,
    disp_send,
    disp_recv,
    hop_send,
    hop_recv,
    first_send,
    first_recv,
    halo_sem,
    conv_sem,
    back_send,
    back_recv,
    last_send,
    last_recv,
):
    tokens, width = raw_m.shape
    C = value_w.shape[1]
    F = gate_w.shape[1]
    half = EP // 2
    rows = half * 2 * CAP
    piece = width // PIECES
    hops = Z // 2

    e = lax.axis_index("ep")
    tp = lax.axis_index("tp")
    z, c = tp // 2, lax.rem(tp, 2)
    ep_odd = lax.rem(e, 2)
    slot = e // 2
    partner = (e, z * 2 + 1 - c)

    def to_expert(i):
        return (2 * i + c, z * 2 + 1 - ep_odd)

    def to_source(i):
        return (2 * i + 1 - c, z * 2 + ep_odd)

    def beside(step):
        return (e, lax.rem(z + step + Z, Z) * 2 + c)

    def remote(src, dst, ssem, rsem, device):
        return pltpu.make_async_remote_copy(
            src_ref=src, dst_ref=dst, send_sem=ssem, recv_sem=rsem, device_id=device, device_id_type=MESH
        )

    home = 2 * SHARE

    def home_of(s):
        k = (s + 1) // 2
        sign = 2 * lax.rem(s, 2) - 1
        return lax.rem(z + jnp.where(s == 0, hops, sign * (hops - k)) + Z, Z)

    def token_load(s):
        span = pl.ds(pl.multiple_of(home_of(s) * home, home), home)
        return pltpu.make_async_copy(moe_x.at[span], raw_e.at[span], tok_sem.at[s])

    token_load(0).start()
    loads = [
        pltpu.make_async_copy(src, dst, load_sem.at[n])
        for n, (src, dst) in enumerate(
            [
                (mix_x, raw_m),
                (value_w, proj_w.at[:, 0:C]),
                (inner_w, proj_w.at[:, C : 2 * C]),
                (outer_w, proj_w.at[:, 2 * C : 3 * C]),
                (mix_w, mixw.at[0:C]),
                (gate_w, gu_w.at[:, 0:F]),
                (up_w, gu_w.at[:, 2 * F : 3 * F]),
                (down_w, dn_w.at[0:F]),
            ]
        )
    ]
    barrier = pltpu.get_barrier_semaphore()
    greet = [to_expert(i) for i in range(half)] + [to_source(i) for i in range(half)]
    greet += [beside(1), beside(-1)]
    greet += [(lax.rem(e + 1, EP), tp), (lax.rem(e + EP - 1, EP), tp)]
    for device in greet:
        pl.semaphore_signal(barrier, inc=1, device_id=device, device_id_type=MESH)
    for copy in loads[0:4]:
        copy.start()

    def load_tokens(s, carry):
        token_load(s).start()
        return carry

    lax.fori_loop(1, Z, load_tokens, 0)
    for copy in loads[4:]:
        copy.start()

    row = lax.broadcasted_iota(jnp.int32, (rows, home), 0)
    tok = lax.broadcasted_iota(jnp.int32, (rows, home), 1)
    expert_of = (2 * (row >> 3) + c).astype(F32)
    slot_of = (row & 3).astype(F32)
    in_block = (tok >> 4) == ((row >> 2) & 1)
    bef_r = lax.broadcasted_iota(jnp.int32, (home, home), 0)
    bef_c = lax.broadcasted_iota(jnp.int32, (home, home), 1)
    before = ((bef_r < bef_c) & ((bef_r >> 4) == (bef_c >> 4))).astype(F32).astype(BF16)
    pick_r = lax.broadcasted_iota(jnp.int32, (tokens, home), 0)
    pick_c = lax.broadcasted_iota(jnp.int32, (tokens, home), 1)
    routes_b = routes[...].astype(F32).astype(BF16)

    def routed(zh):
        pick = (pick_r == pick_c + zh * home).astype(F32).astype(BF16)
        named = jnp.dot(routes_b, pick, preferred_element_type=F32)
        h0, h1 = named[0:1, :], named[1:2, :]
        is0, is1 = h0 == expert_of, h1 == expert_of
        rank = jnp.dot((is0 | is1).astype(F32).astype(BF16), before, preferred_element_type=F32)
        at = (rank == slot_of) & in_block
        return h0, h1, at & is0, at & is1

    def dispatch(s):
        for i in range(half):
            remote(send.at[s, i], recv.at[s, slot], disp_send.at[s], disp_recv.at[s], to_expert(i)).start()

    def place(s):
        zh = home_of(s)
        _, _, at0, at1 = routed(zh)
        chosen = (at0 | at1).astype(F32).astype(BF16)
        start = pl.multiple_of(zh * home, home)
        token_load(s).wait()
        rms_rows(raw_e, moe_gain[...], norm_e, start, home)

        def columns(n, carry):
            cols = pl.ds(pl.multiple_of(n * 512, 512), 512)
            placed = jnp.dot(chosen, norm_e[pl.ds(start, home), cols], preferred_element_type=F32)
            send[s, :, :, cols] = placed.reshape(half, 2 * CAP, 512).astype(BF16)
            return carry

        lax.fori_loop(0, width // 512, columns, 0)

        @pl.when(s == 0)
        def _():
            pl.semaphore_wait(barrier, len(greet))

        dispatch(s)

    swaps = [
        remote(src, dst, swap_send.at[n], swap_recv.at[n], partner)
        for n, (src, dst) in enumerate(
            [
                (gate_w, gu_w.at[:, F : 2 * F]),
                (up_w, gu_w.at[:, 3 * F : 4 * F]),
                (mix_w, mixw.at[C : 2 * C]),
                (down_w, dn_w.at[F : 2 * F]),
            ]
        )
    ]
    halo = remote(halo_out, halo_in, halo_sem.at[0], halo_sem.at[1], (lax.rem(e + 1, EP), tp))
    conv_swap = remote(conv.at[1 - c], conv_all.at[:, C : 2 * C], conv_sem.at[0], conv_sem.at[1], partner)

    def mixer_head():
        loads[0].wait()
        rms_rows(raw_m, mix_gain[...], norm_m, 0, tokens)
        for n in (1, 2, 3):
            loads[n].wait()
        proj = jnp.dot(norm_m[...], proj_w[...], preferred_element_type=F32)
        gated_in = (proj[:, C : 2 * C] * proj[:, 0:C]).astype(BF16)
        outer_p[...] = proj[:, 2 * C : 3 * C]
        gated[pl.ds(SHARE, tokens), :] = gated_in.astype(F32)
        halo_out[...] = gated_in[tokens - SHARE :, :]
        halo.start()

    def mixer_conv():
        halo.wait()
        gated[0:SHARE, :] = jnp.where(e > 0, halo_in[...].astype(F32), 0.0)
        mixed = taps[0:1, :] * gated[pl.ds(SHARE - 2, tokens), :]
        mixed = mixed + taps[1:2, :] * gated[pl.ds(SHARE - 1, tokens), :]
        mixed = mixed + taps[2:3, :] * gated[pl.ds(SHARE, tokens), :]
        conv_out = (outer_p[...] * mixed).astype(BF16).reshape(Z, 2, SHARE, C)
        conv[0] = conv_out[:, 0].reshape(Z * SHARE, C)
        conv[1] = conv_out[:, 1].reshape(Z * SHARE, C)
        conv_swap.start()
        conv_all[:, 0:C] = conv[c]

    def first_mix(j):
        side = 1 if j < PIECES // 2 else 0
        return remote(
            rs_send.at[side, 0, j, rows:],
            rs_recv.at[side, 0, j, rows:],
            first_send.at[j],
            first_recv.at[j],
            beside(2 * side - 1),
        )

    def mixer_down():
        loads[4].wait()
        swaps[2].wait_recv()
        conv_swap.wait()

        def down_mix(n, carry):
            cols = pl.ds(pl.multiple_of(n * 512, 512), 512)
            part = jnp.dot(conv_all[...], mixw[:, cols], preferred_element_type=F32)
            mix_part[:, :, cols] = part.reshape(Z, SHARE, 512)
            return carry

        lax.fori_loop(0, width // 512, down_mix, 0)
        far = home_of(0)
        for j in range(PIECES):
            side = 1 if j < PIECES // 2 else 0
            rs_send[side, 0, j, rows:, :] = mix_part[far, :, j * piece : (j + 1) * piece].astype(BF16)
            first_mix(j).start()

    def weigh():
        h0, h1, at0, at1 = routed(z)
        own_normed = norm_e[pl.ds(pl.multiple_of(z * home, home), home), :]
        contract_last = (((1,), (1,)), ((), ()))
        group_logit = lax.dot_general(router_g[...], own_normed, contract_last, preferred_element_type=F32)
        expert_logit = lax.dot_general(router_e[...], own_normed, contract_last, preferred_element_type=F32)
        group_exp = jnp.exp(group_logit)
        first_of = (lax.broadcasted_iota(jnp.int32, group_exp.shape, 0) * EPG).astype(F32)
        in_group = (h0 >= first_of) & (h0 < first_of + EPG)
        gate = jnp.sum(jnp.where(in_group, group_exp, 0.0), axis=0, keepdims=True) / jnp.sum(
            group_exp, axis=0, keepdims=True
        )
        number = lax.broadcasted_iota(jnp.int32, expert_logit.shape, 0).astype(F32)
        chosen0 = jnp.exp(jnp.sum(jnp.where(number == h0, expert_logit, 0.0), axis=0, keepdims=True))
        chosen1 = jnp.exp(jnp.sum(jnp.where(number == h1, expert_logit, 0.0), axis=0, keepdims=True))
        both = chosen0 + chosen1
        weight = jnp.where(at0, gate * chosen0 / both, 0.0) + jnp.where(at1, gate * chosen1 / both, 0.0)
        weight = weight.T
        high = weight.astype(BF16)
        comb_w[0:home, :] = high
        comb_w[home : 2 * home, :] = (weight - high.astype(F32)).astype(BF16)

    def hop(direction, k, j):
        return remote(
            rs_send.at[direction, k, j],
            rs_recv.at[direction, k, j],
            hop_send.at[direction, k, j],
            hop_recv.at[direction, k, j],
            beside(2 * direction - 1),
        )

    def give_back(j, i):
        return remote(ret_send.at[j, i], ret_recv.at[j, slot], back_send.at[j], back_recv.at[j], to_source(i))

    def first_rows(j):
        side = 1 if j < PIECES // 2 else 0
        return remote(
            rs_send.at[side, 0, j, 0:rows],
            rs_recv.at[side, 0, j, 0:rows],
            hop_send.at[side, 0, j],
            hop_recv.at[side, 0, j],
            beside(2 * side - 1),
        )

    def stage(s, carry):
        @pl.when(s + AHEAD < Z)
        def _():
            place(s + AHEAD)

        @pl.when(s == 0)
        def _():
            mixer_conv()
            for n in (5, 6, 7):
                loads[n].wait()
            for n in (0, 1, 3):
                swaps[n].wait_recv()

        @pl.when(s == 1)
        def _():
            mixer_down()

        @pl.when(s == Z - AHEAD)
        def _():
            weigh()

        arrived = remote(send.at[s], recv.at[s], disp_send.at[s], disp_recv.at[s], partner)
        arrived.wait_recv()
        x = recv[s].reshape(rows, width)
        gate_up = jnp.dot(x, gu_w[...], preferred_element_type=F32)
        g, u = gate_up[:, 0 : 2 * F], gate_up[:, 2 * F :]
        hidden = (g / (1.0 + jnp.exp(-g)) * u).astype(BF16)
        direction = lax.rem(s, 2)
        k = (s + 1) // 2
        zs = home_of(s)
        for j in range(PIECES):
            cols = slice(j * piece, (j + 1) * piece)
            side = 1 if j < PIECES // 2 else 0
            acc[0:rows, :] = jnp.dot(hidden, dn_w[:, cols], preferred_element_type=F32)

            @pl.when(s == 0)
            def _():
                rs_send[side, 0, j, 0:rows, :] = acc[0:rows, :].astype(BF16)
                first_rows(j).start()

            @pl.when((s > 0) & (s < Z - 1))
            def _():
                acc[rows:, :] = mix_part[zs, :, cols]

                @pl.when((k == 1) & (direction == side))
                def _():
                    first_rows(j).wait_recv()
                    first_mix(j).wait_recv()
                    acc[...] += rs_recv[side, 0, j].astype(F32)

                @pl.when(k > 1)
                def _():
                    hop(direction, k - 1, j).wait_recv()
                    acc[...] += rs_recv[direction, k - 1, j].astype(F32)

                rs_send[direction, k, j] = acc[...].astype(BF16)
                hop(direction, k, j).start()

            @pl.when(s == Z - 1)
            def _():
                acc[rows:, :] = mix_part[zs, :, cols]
                for way in (1, 0):
                    hop(way, hops - 1, j).wait_recv()
                    acc[...] += rs_recv[way, hops - 1, j].astype(F32)
                ret_send[j] = acc[0:rows, :].astype(BF16).reshape(half, 2 * CAP, piece)
                for i in range(half):
                    give_back(j, i).start()
                mix_out[:, cols] = acc[rows:, :].astype(BF16)

        return carry

    place(jnp.int32(0))
    for copy in swaps:
        copy.start()
    mixer_head()

    def place_early(s, carry):
        place(s)
        return carry

    lax.fori_loop(1, AHEAD, place_early, 0)
    lax.fori_loop(0, Z, stage, 0)

    def last(j):
        return remote(comb.at[j, 1 - c], comb_in.at[j], last_send.at[j], last_recv.at[j], partner)

    for j in range(PIECES):
        remote(ret_send.at[j], ret_recv.at[j], back_send.at[j], back_recv.at[j], partner).wait_recv()
        summed = jnp.dot(comb_w[...], ret_recv[j].reshape(rows, piece), preferred_element_type=F32)
        comb[j] = (summed[0:home] + summed[home:]).reshape(2, SHARE, piece)
        last(j).start()
    for j in range(PIECES):
        last(j).wait_recv()
        moe_out[:, j * piece : (j + 1) * piece] = (comb[j, c] + comb_in[j]).astype(BF16)

    for copy in swaps:
        copy.wait_send()
    for s in range(Z):
        remote(send.at[s], recv.at[s], disp_send.at[s], disp_recv.at[s], partner).wait_send()
    for j in range(PIECES):
        first_rows(j).wait_send()
        first_mix(j).wait_send()
        for k in range(1, hops):
            for direction in (0, 1):
                hop(direction, k, j).wait_send()
        remote(ret_send.at[j], ret_recv.at[j], back_send.at[j], back_recv.at[j], partner).wait_send()
        last(j).wait_send()


def solution(mesh):
    EP, TP = mesh.shape["ep"], mesh.shape["tp"]
    Z = TP // 2

    def local(
        mix_tokens,
        mix_gain,
        value_weight,
        inner_weight,
        outer_weight,
        conv_taps,
        mix_weight,
        moe_tokens,
        moe_gain,
        router_group,
        router_expert,
        expert_routes,
        gate_weight,
        up_weight,
        down_weight,
    ):
        tokens, D = mix_tokens.shape
        C = value_weight.shape[1]
        F = gate_weight.shape[2]
        half = EP // 2
        rows = half * 2 * CAP
        piece = D // PIECES
        hops = Z // 2
        vmem = pl.BlockSpec(memory_space=pltpu.VMEM)
        hbm = pl.BlockSpec(memory_space=pl.ANY)
        V = pltpu.VMEM
        DMA = pltpu.SemaphoreType.DMA
        out = jax.ShapeDtypeStruct((SHARE, D), BF16)
        return pl.pallas_call(
            functools.partial(kernel, EP, Z),
            out_shape=(out, out),
            in_specs=[hbm, vmem, hbm, hbm, hbm, vmem, hbm, hbm, vmem, vmem, vmem, vmem, hbm, hbm, hbm],
            out_specs=(vmem, vmem),
            scratch_shapes=[
                V((tokens, D), BF16),
                V((tokens, D), BF16),
                V((tokens, D), BF16),
                V((tokens, D), BF16),
                V((D, 4 * F), BF16),
                V((2 * F, D), BF16),
                V((D, 3 * C), BF16),
                V((2 * C, D), BF16),
                V((Z, half, 2 * CAP, D), BF16),
                V((Z, half, 2 * CAP, D), BF16),
                V((rows + SHARE, piece), F32),
                V((2, hops, PIECES, rows + SHARE, piece), BF16),
                V((2, hops, PIECES, rows + SHARE, piece), BF16),
                V((SHARE, C), BF16),
                V((SHARE, C), BF16),
                V((SHARE + tokens, C), F32),
                V((tokens, C), F32),
                V((2, Z * SHARE, C), BF16),
                V((Z * SHARE, 2 * C), BF16),
                V((Z, SHARE, D), F32),
                V((4 * SHARE, rows), BF16),
                V((PIECES, half, 2 * CAP, piece), BF16),
                V((PIECES, half, 2 * CAP, piece), BF16),
                V((PIECES, 2, SHARE, piece), F32),
                V((PIECES, SHARE, piece), F32),
                DMA((8,)),
                DMA((Z,)),
                DMA((4,)),
                DMA((4,)),
                DMA((Z,)),
                DMA((Z,)),
                DMA((2, hops, PIECES)),
                DMA((2, hops, PIECES)),
                DMA((PIECES,)),
                DMA((PIECES,)),
                DMA((2,)),
                DMA((2,)),
                DMA((PIECES,)),
                DMA((PIECES,)),
                DMA((PIECES,)),
                DMA((PIECES,)),
            ],
            compiler_params=pltpu.CompilerParams(
                collective_id=0, has_side_effects=True, vmem_limit_bytes=60 * 1024 * 1024
            ),
            name="mixer_and_experts",
        )(
            mix_tokens,
            mix_gain.reshape(1, D),
            value_weight,
            inner_weight,
            outer_weight,
            conv_taps,
            mix_weight,
            moe_tokens,
            moe_gain.reshape(1, D),
            router_group.T,
            router_expert.T,
            expert_routes.T,
            gate_weight.reshape(D, F),
            up_weight.reshape(D, F),
            down_weight.reshape(F, D),
        )

    return jax.shard_map(
        local,
        mesh=mesh,
        in_specs=(
            P("ep", None),
            P(),
            P(None, "tp"),
            P(None, "tp"),
            P(None, "tp"),
            P(None, "tp"),
            P("tp", None),
            P("ep", None),
            P(),
            P(),
            P(),
            P("ep", None),
            P("ep", None, "tp"),
            P("ep", None, "tp"),
            P("ep", "tp", None),
        ),
        out_specs=(P(("ep", "tp"), None), P(("ep", "tp"), None)),
        check_vma=False,
    )
```

```python
import functools

import jax
import jax.numpy as jnp
from jax import lax
from jax.experimental import pallas as pl
from jax.experimental.pallas import tpu as pltpu
from jax.sharding import PartitionSpec as P

MESH = pl.DeviceIdType.MESH
F32 = jnp.float32
BF16 = jnp.bfloat16
SHARE = 16
CAP = 4
EPG = 4
EPS = 1e-06
PIECES = 4
WIDE = 2048
LATER = 1
VMEM_MIB = 60
SIDE = 4
AHEAD = 3


def rms_rows(raw, gain, out, start, count):
    def body(i, carry):
        rows = pl.ds(pl.multiple_of(start + i * SHARE, SHARE), SHARE)
        values = raw[rows, :].astype(F32)
        inverse = lax.rsqrt(jnp.mean(values * values, axis=-1, keepdims=True) + EPS)
        out[rows, :] = (values * inverse * gain).astype(BF16)
        return carry

    lax.fori_loop(0, count // SHARE, body, 0)


def kernel(
    EP,
    Z,
    mix_x,
    mix_gain_h,
    value_w,
    inner_w,
    outer_w,
    taps_h,
    mix_w,
    moe_x,
    moe_gain_h,
    router_g_h,
    router_e_h,
    routes_h,
    gate_w,
    up_w,
    down_w,
    mix_out,
    moe_out,
    mix_gain,
    taps,
    moe_gain,
    router_g,
    router_e,
    routes,
    raw_m,
    raw_e,
    norm_m,
    norm_e,
    gu_w,
    dn_w,
    proj_w,
    mixw,
    send,
    recv,
    acc,
    rs_send,
    rs_recv,
    mix_send,
    mix_recv,
    halo_out,
    halo_in,
    gated,
    outer_p,
    conv,
    conv_all,
    mix_part,
    comb_w,
    ret_send,
    ret_recv,
    comb,
    comb_in,
    load_sem,
    tok_sem,
    small_sem,
    swap_send,
    swap_recv,
    disp_send,
    disp_recv,
    credit,
    hop_send,
    hop_recv,
    mixhop_send,
    mixhop_recv,
    halo_sem,
    conv_sem,
    back_send,
    back_recv,
    last_send,
    last_recv,
):
    tokens, width = raw_m.shape
    C = value_w.shape[1]
    F = gate_w.shape[1]
    half = EP // 2
    rows = half * 2 * CAP
    piece = width // PIECES
    hops = Z // 2

    e = lax.axis_index("ep")
    tp = lax.axis_index("tp")
    z, c = tp // 2, lax.rem(tp, 2)
    ep_odd = lax.rem(e, 2)
    slot = e // 2
    partner = (e, z * 2 + 1 - c)

    def to_expert(i):
        return (2 * i + c, z * 2 + 1 - ep_odd)

    def to_source(i):
        return (2 * i + 1 - c, z * 2 + ep_odd)

    def beside(step):
        return (e, lax.rem(z + step + Z, Z) * 2 + c)

    def remote(src, dst, ssem, rsem, device):
        return pltpu.make_async_remote_copy(
            src_ref=src, dst_ref=dst, send_sem=ssem, recv_sem=rsem, device_id=device, device_id_type=MESH
        )

    home = 2 * SHARE

    def home_of(s):
        k = (s + 1) // 2
        sign = 2 * lax.rem(s, 2) - 1
        return lax.rem(z + jnp.where(s == 0, hops, sign * (hops - k)) + Z, Z)

    def token_load(s):
        span = pl.ds(pl.multiple_of(home_of(s) * home, home), home)
        return pltpu.make_async_copy(moe_x.at[span], raw_e.at[span], tok_sem.at[s])

    smalls = [
        pltpu.make_async_copy(src, dst, small_sem.at[n])
        for n, (src, dst) in enumerate(
            [
                (routes_h, routes),
                (moe_gain_h, moe_gain),
                (mix_gain_h, mix_gain),
                (taps_h, taps),
                (router_g_h, router_g),
                (router_e_h, router_e),
            ]
        )
    ]
    loads = [
        pltpu.make_async_copy(src, dst, load_sem.at[n])
        for n, (src, dst) in enumerate(
            [
                (mix_x, raw_m),
                (value_w, proj_w.at[:, 0:C]),
                (inner_w, proj_w.at[:, C : 2 * C]),
                (outer_w, proj_w.at[:, 2 * C : 3 * C]),
                (mix_w, mixw.at[0:C]),
                (gate_w, gu_w.at[:, 0:F]),
                (up_w, gu_w.at[:, 2 * F : 3 * F]),
                (down_w, dn_w.at[0:F]),
            ]
        )
    ]
    smalls[0].start()
    token_load(0).start()
    smalls[1].start()
    barrier = pltpu.get_barrier_semaphore()
    greet = [to_expert(i) for i in range(half)] + [to_source(i) for i in range(half)]
    greet += [beside(1), beside(-1)]
    greet += [(lax.rem(e + 1, EP), tp), (lax.rem(e + EP - 1, EP), tp)]
    for device in greet:
        pl.semaphore_signal(barrier, inc=1, device_id=device, device_id_type=MESH)
    smalls[2].start()
    for copy in loads[0:4]:
        copy.start()

    def load_tokens(s, carry):
        token_load(s).start()
        return carry

    lax.fori_loop(1, Z, load_tokens, 0)
    for copy in loads[4:] + smalls[3:]:
        copy.start()

    row = lax.broadcasted_iota(jnp.int32, (rows, home), 0)
    tok = lax.broadcasted_iota(jnp.int32, (rows, home), 1)
    expert_of = (2 * (row >> 3) + c).astype(F32)
    slot_of = (row & 3).astype(F32)
    in_block = (tok >> 4) == ((row >> 2) & 1)
    bef_r = lax.broadcasted_iota(jnp.int32, (home, home), 0)
    bef_c = lax.broadcasted_iota(jnp.int32, (home, home), 1)
    before = ((bef_r < bef_c) & ((bef_r >> 4) == (bef_c >> 4))).astype(F32).astype(BF16)
    pick_r = lax.broadcasted_iota(jnp.int32, (tokens, home), 0)
    pick_c = lax.broadcasted_iota(jnp.int32, (tokens, home), 1)
    smalls[0].wait()
    routes_b = routes[...].astype(F32).astype(BF16)

    def routed(zh):
        pick = (pick_r == pick_c + zh * home).astype(F32).astype(BF16)
        named = jnp.dot(routes_b, pick, preferred_element_type=F32)
        h0, h1 = named[0:1, :], named[1:2, :]
        is0, is1 = h0 == expert_of, h1 == expert_of
        rank = jnp.dot((is0 | is1).astype(F32).astype(BF16), before, preferred_element_type=F32)
        at = (rank == slot_of) & in_block
        return h0, h1, at & is0, at & is1

    def dispatch(s):
        y, x = e // SIDE, lax.rem(e, SIDE)
        odd = lax.rem(c + x, 2)
        for dy in (2, 1, 3, 0):
            for n in (0, 1):
                dx = 2 - 2 * n + odd * (4 * n - 1)
                i = (lax.rem(y + dy, SIDE) * SIDE + lax.rem(x + dx, SIDE)) // 2
                remote(send.at[s, i], recv.at[s, slot], disp_send.at[s], disp_recv.at[s], to_expert(i)).start()

    def place(s):
        zh = home_of(s)
        _, _, at0, at1 = routed(zh)
        chosen = (at0 | at1).astype(F32).astype(BF16)
        start = pl.multiple_of(zh * home, home)
        token_load(s).wait()
        rms_rows(raw_e, moe_gain[...], norm_e, start, home)
        for n in range(width // WIDE):
            cols = slice(n * WIDE, (n + 1) * WIDE)
            placed = jnp.dot(chosen, norm_e[pl.ds(start, home), cols], preferred_element_type=F32)
            send[s, :, :, cols] = placed.reshape(half, 2 * CAP, WIDE).astype(BF16)

    swaps = [
        remote(src, dst, swap_send.at[n], swap_recv.at[n], partner)
        for n, (src, dst) in enumerate(
            [
                (gate_w, gu_w.at[:, F : 2 * F]),
                (up_w, gu_w.at[:, 3 * F : 4 * F]),
                (mix_w, mixw.at[C : 2 * C]),
                (down_w, dn_w.at[F : 2 * F]),
            ]
        )
    ]
    halo = remote(halo_out, halo_in, halo_sem.at[0], halo_sem.at[1], (lax.rem(e + 1, EP), tp))
    conv_swap = remote(conv.at[1 - c], conv_all.at[:, C : 2 * C], conv_sem.at[0], conv_sem.at[1], partner)

    def mixer_tail():
        smalls[2].wait()
        loads[0].wait()
        rms_rows(raw_m, mix_gain[...], norm_m, tokens - SHARE, SHARE)
        for n in (1, 2):
            loads[n].wait()
        tail = jnp.dot(norm_m[tokens - SHARE :, :], proj_w[:, 0 : 2 * C], preferred_element_type=F32)
        halo_out[...] = (tail[:, C:] * tail[:, 0:C]).astype(BF16)

    def mixer_proj():
        rms_rows(raw_m, mix_gain[...], norm_m, 0, tokens - SHARE)
        loads[3].wait()
        proj = jnp.dot(norm_m[...], proj_w[...], preferred_element_type=F32)
        gated_in = (proj[:, C : 2 * C] * proj[:, 0:C]).astype(BF16)
        outer_p[...] = proj[:, 2 * C : 3 * C]
        gated[pl.ds(SHARE, tokens), :] = gated_in.astype(F32)

    def mixer_conv():
        halo.wait()
        smalls[3].wait()
        gated[0:SHARE, :] = jnp.where(e > 0, halo_in[...].astype(F32), 0.0)
        mixed = taps[0:1, :] * gated[pl.ds(SHARE - 2, tokens), :]
        mixed = mixed + taps[1:2, :] * gated[pl.ds(SHARE - 1, tokens), :]
        mixed = mixed + taps[2:3, :] * gated[pl.ds(SHARE, tokens), :]
        conv_out = (outer_p[...] * mixed).astype(BF16).reshape(Z, 2, SHARE, C)
        conv[0] = conv_out[:, 0].reshape(Z * SHARE, C)
        conv[1] = conv_out[:, 1].reshape(Z * SHARE, C)
        conv_swap.start()
        swaps[3].start()
        conv_all[:, 0:C] = conv[c]

    def mix_hop(direction, k):
        if k == 0:
            part = 1 - direction
            src, dst = mix_send.at[direction, 0, part], mix_recv.at[direction, 0, part]
        else:
            src, dst = mix_send.at[direction, k], mix_recv.at[direction, k]
        return remote(
            src, dst, mixhop_send.at[direction, k], mixhop_recv.at[direction, k], beside(2 * direction - 1)
        )

    def mixer_hop(k):
        for direction in (1, 0):
            zh = lax.rem(z + (2 * direction - 1) * (hops - k) + Z, Z)
            if k:
                mix_hop(direction, k - 1).wait_recv()
            for part in (0, 1):
                total = mix_part[zh, :, part * (width // 2) : (part + 1) * (width // 2)]
                if k == 0 and part == direction:
                    continue
                if k > 1 or (k == 1 and part != direction):
                    total = total + mix_recv[direction, k - 1, part].astype(F32)
                mix_send[direction, k, part] = total.astype(BF16)
            mix_hop(direction, k).start()

    def mixer_end():
        for direction in (1, 0):
            mix_hop(direction, hops - 1).wait_recv()
        for part in (0, 1):
            cols = slice(part * (width // 2), (part + 1) * (width // 2))
            total = mix_part[z, :, cols] + mix_recv[1, hops - 1, part].astype(F32)
            mix_out[:, cols] = (total + mix_recv[0, hops - 1, part].astype(F32)).astype(BF16)

    def mixer_down():
        loads[4].wait()
        swaps[2].wait_recv()
        conv_swap.wait()

        def down_mix(n, carry):
            cols = pl.ds(pl.multiple_of(n * 512, 512), 512)
            part = jnp.dot(conv_all[...], mixw[:, cols], preferred_element_type=F32)
            mix_part[:, :, cols] = part.reshape(Z, SHARE, 512)
            return carry

        lax.fori_loop(0, width // 512, down_mix, 0)
        mixer_hop(0)

    def weigh():
        smalls[4].wait()
        smalls[5].wait()
        h0, h1, at0, at1 = routed(z)
        own_normed = norm_e[pl.ds(pl.multiple_of(z * home, home), home), :]
        contract_last = (((1,), (1,)), ((), ()))
        group_logit = lax.dot_general(router_g[...], own_normed, contract_last, preferred_element_type=F32)
        expert_logit = lax.dot_general(router_e[...], own_normed, contract_last, preferred_element_type=F32)
        group_exp = jnp.exp(group_logit)
        first_of = (lax.broadcasted_iota(jnp.int32, group_exp.shape, 0) * EPG).astype(F32)
        in_group = (h0 >= first_of) & (h0 < first_of + EPG)
        gate = jnp.sum(jnp.where(in_group, group_exp, 0.0), axis=0, keepdims=True) / jnp.sum(
            group_exp, axis=0, keepdims=True
        )
        number = lax.broadcasted_iota(jnp.int32, expert_logit.shape, 0).astype(F32)
        chosen0 = jnp.exp(jnp.sum(jnp.where(number == h0, expert_logit, 0.0), axis=0, keepdims=True))
        chosen1 = jnp.exp(jnp.sum(jnp.where(number == h1, expert_logit, 0.0), axis=0, keepdims=True))
        both = chosen0 + chosen1
        weight = jnp.where(at0, gate * chosen0 / both, 0.0) + jnp.where(at1, gate * chosen1 / both, 0.0)
        weight = weight.T
        high = weight.astype(BF16)
        comb_w[0:home, :] = high
        comb_w[home : 2 * home, :] = (weight - high.astype(F32)).astype(BF16)

    def hop(direction, k, j):
        return remote(
            rs_send.at[direction, k, j],
            rs_recv.at[direction, k, j],
            hop_send.at[direction, k, j],
            hop_recv.at[direction, k, j],
            beside(2 * direction - 1),
        )

    def give_back(j, i):
        return remote(ret_send.at[j, i], ret_recv.at[j, slot], back_send.at[j], back_recv.at[j], to_source(i))

    def first_rows(j):
        side = 1 if j < PIECES // 2 else 0
        return remote(
            rs_send.at[side, 0, j],
            rs_recv.at[side, 0, j],
            hop_send.at[side, 0, j],
            hop_recv.at[side, 0, j],
            beside(2 * side - 1),
        )

    def stage(s, carry):
        @pl.when((s > 0) & (s - 1 + AHEAD < Z))
        def _():
            place(s - 1 + AHEAD)
            pl.semaphore_wait(credit.at[s - 1], half)
            dispatch(s - 1 + AHEAD)

        @pl.when(s == 0)
        def _():
            mixer_down()
            for n in (5, 6, 7):
                loads[n].wait()
            for n in (0, 1, 3):
                swaps[n].wait_recv()

        for k in range(1, hops):

            @pl.when(s == (k if k < 3 else k + LATER))
            def _():
                mixer_hop(k)

        @pl.when(s == Z - 1)
        def _():
            mixer_end()

        @pl.when(s == Z + 1 - AHEAD)
        def _():
            weigh()

        arrived = remote(send.at[s], recv.at[s], disp_send.at[s], disp_recv.at[s], partner)
        arrived.wait_recv()

        @pl.when(s + AHEAD < Z)
        def _():
            for i in range(half):
                pl.semaphore_signal(credit.at[s], inc=1, device_id=to_source(i), device_id_type=MESH)

        x = recv[s].reshape(rows, width)
        gate_up = jnp.dot(x, gu_w[...], preferred_element_type=F32)
        g, u = gate_up[:, 0 : 2 * F], gate_up[:, 2 * F :]
        hidden = (g / (1.0 + jnp.exp(-g)) * u).astype(BF16)
        direction = lax.rem(s, 2)
        k = (s + 1) // 2
        for j in range(PIECES):
            cols = slice(j * piece, (j + 1) * piece)
            side = 1 if j < PIECES // 2 else 0
            acc[...] = jnp.dot(hidden, dn_w[:, cols], preferred_element_type=F32)

            @pl.when(s == 0)
            def _():
                rs_send[side, 0, j] = acc[...].astype(BF16)
                first_rows(j).start()

            @pl.when((s > 0) & (s < Z - 1))
            def _():
                @pl.when((k == 1) & (direction == side))
                def _():
                    first_rows(j).wait_recv()
                    acc[...] += rs_recv[side, 0, j].astype(F32)

                @pl.when(k > 1)
                def _():
                    hop(direction, k - 1, j).wait_recv()
                    acc[...] += rs_recv[direction, k - 1, j].astype(F32)

                rs_send[direction, k, j] = acc[...].astype(BF16)
                hop(direction, k, j).start()

            @pl.when(s == Z - 1)
            def _():
                for way in (1, 0):
                    hop(way, hops - 1, j).wait_recv()
                    acc[...] += rs_recv[way, hops - 1, j].astype(F32)
                ret_send[j] = acc[...].astype(BF16).reshape(half, 2 * CAP, piece)
                for i in range(half):
                    give_back(j, i).start()

        return carry

    smalls[1].wait()
    place(jnp.int32(0))
    mixer_tail()
    pl.semaphore_wait(barrier, len(greet))
    halo.start()
    dispatch(jnp.int32(0))
    for n in (2, 0, 1):
        swaps[n].start()
    mixer_proj()

    def place_early(s, carry):
        place(s)
        dispatch(s)
        return carry

    lax.fori_loop(1, AHEAD, place_early, 0)
    mixer_conv()
    lax.fori_loop(0, Z, stage, 0)

    def last(j):
        return remote(comb.at[j, 1 - c], comb_in.at[j], last_send.at[j], last_recv.at[j], partner)

    for j in range(PIECES):
        remote(ret_send.at[j], ret_recv.at[j], back_send.at[j], back_recv.at[j], partner).wait_recv()
        summed = jnp.dot(comb_w[...], ret_recv[j].reshape(rows, piece), preferred_element_type=F32)
        comb[j] = (summed[0:home] + summed[home:]).reshape(2, SHARE, piece)
        last(j).start()
    for j in range(PIECES):
        last(j).wait_recv()
        moe_out[:, j * piece : (j + 1) * piece] = (comb[j, c] + comb_in[j]).astype(BF16)

    for copy in swaps:
        copy.wait_send()
    for k in range(hops):
        for direction in (0, 1):
            mix_hop(direction, k).wait_send()
    for s in range(Z):
        remote(send.at[s], recv.at[s], disp_send.at[s], disp_recv.at[s], partner).wait_send()
    for j in range(PIECES):
        first_rows(j).wait_send()
        for k in range(1, hops):
            for direction in (0, 1):
                hop(direction, k, j).wait_send()
        remote(ret_send.at[j], ret_recv.at[j], back_send.at[j], back_recv.at[j], partner).wait_send()
        last(j).wait_send()


def solution(mesh):
    EP, TP = mesh.shape["ep"], mesh.shape["tp"]
    Z = TP // 2

    def local(
        mix_tokens,
        mix_gain,
        value_weight,
        inner_weight,
        outer_weight,
        conv_taps,
        mix_weight,
        moe_tokens,
        moe_gain,
        router_group,
        router_expert,
        expert_routes,
        gate_weight,
        up_weight,
        down_weight,
    ):
        tokens, D = mix_tokens.shape
        C = value_weight.shape[1]
        F = gate_weight.shape[2]
        half = EP // 2
        rows = half * 2 * CAP
        piece = D // PIECES
        hops = Z // 2
        vmem = pl.BlockSpec(memory_space=pltpu.VMEM)
        hbm = pl.BlockSpec(memory_space=pltpu.HBM)
        V = pltpu.VMEM
        DMA = pltpu.SemaphoreType.DMA
        out = jax.ShapeDtypeStruct((SHARE, D), BF16)
        return pl.pallas_call(
            functools.partial(kernel, EP, Z),
            out_shape=(out, out),
            in_specs=[hbm] * 15,
            out_specs=(vmem, vmem),
            scratch_shapes=[
                V((1, D), F32),
                V(conv_taps.shape, F32),
                V((1, D), F32),
                V((router_group.shape[1], D), BF16),
                V((router_expert.shape[1], D), BF16),
                V((2, tokens), jnp.int32),
                V((tokens, D), BF16),
                V((tokens, D), BF16),
                V((tokens, D), BF16),
                V((tokens, D), BF16),
                V((D, 4 * F), BF16),
                V((2 * F, D), BF16),
                V((D, 3 * C), BF16),
                V((2 * C, D), BF16),
                V((Z, half, 2 * CAP, D), BF16),
                V((Z, half, 2 * CAP, D), BF16),
                V((rows, piece), F32),
                V((2, hops, PIECES, rows, piece), BF16),
                V((2, hops, PIECES, rows, piece), BF16),
                V((2, hops, 2, SHARE, D // 2), BF16),
                V((2, hops, 2, SHARE, D // 2), BF16),
                V((SHARE, C), BF16),
                V((SHARE, C), BF16),
                V((SHARE + tokens, C), F32),
                V((tokens, C), F32),
                V((2, Z * SHARE, C), BF16),
                V((Z * SHARE, 2 * C), BF16),
                V((Z, SHARE, D), F32),
                V((4 * SHARE, rows), BF16),
                V((PIECES, half, 2 * CAP, piece), BF16),
                V((PIECES, half, 2 * CAP, piece), BF16),
                V((PIECES, 2, SHARE, piece), F32),
                V((PIECES, SHARE, piece), F32),
                DMA((8,)),
                DMA((Z,)),
                DMA((6,)),
                DMA((4,)),
                DMA((4,)),
                DMA((Z,)),
                DMA((Z,)),
                pltpu.SemaphoreType.REGULAR((Z,)),
                DMA((2, hops, PIECES)),
                DMA((2, hops, PIECES)),
                DMA((2, hops)),
                DMA((2, hops)),
                DMA((2,)),
                DMA((2,)),
                DMA((PIECES,)),
                DMA((PIECES,)),
                DMA((PIECES,)),
                DMA((PIECES,)),
            ],
            compiler_params=pltpu.CompilerParams(
                collective_id=0, has_side_effects=True, vmem_limit_bytes=VMEM_MIB * 1024 * 1024
            ),
            name="mixer_and_experts",
        )(
            mix_tokens,
            mix_gain.reshape(1, D),
            value_weight,
            inner_weight,
            outer_weight,
            conv_taps,
            mix_weight,
            moe_tokens,
            moe_gain.reshape(1, D),
            router_group.T,
            router_expert.T,
            expert_routes.T,
            gate_weight.reshape(D, F),
            up_weight.reshape(D, F),
            down_weight.reshape(F, D),
        )

    return jax.shard_map(
        local,
        mesh=mesh,
        in_specs=(
            P("ep", None),
            P(),
            P(None, "tp"),
            P(None, "tp"),
            P(None, "tp"),
            P(None, "tp"),
            P("tp", None),
            P("ep", None),
            P(),
            P(),
            P(),
            P("ep", None),
            P("ep", None, "tp"),
            P("ep", None, "tp"),
            P("ep", "tp", None),
        ),
        out_specs=(P(("ep", "tp"), None), P(("ep", "tp"), None)),
        check_vma=False,
    )
```

```python
import functools

import jax
import jax.numpy as jnp
from jax import lax
from jax.experimental import pallas as pl
from jax.experimental.pallas import tpu as pltpu
from jax.sharding import PartitionSpec as P

MESH = pl.DeviceIdType.MESH
F32 = jnp.float32
BF16 = jnp.bfloat16
SHARE = 16
CAP = 4
EPG = 4
EPS = 1e-06
PIECES = 4
WIDE = 2048
FINE = 1
MIX_HOPS = ((0, 2, 1), (1, 1, 1), (0, 3, 2), (1, 2, 2), (1, 3, 5))
VMEM_MIB = 60
SIDE = 4
AHEAD = 3


def rms_rows(raw, gain, out, start, count):
    def body(i, carry):
        rows = pl.ds(pl.multiple_of(start + i * SHARE, SHARE), SHARE)
        values = raw[rows, :].astype(F32)
        inverse = lax.rsqrt(jnp.mean(values * values, axis=-1, keepdims=True) + EPS)
        out[rows, :] = (values * inverse * gain).astype(BF16)
        return carry

    lax.fori_loop(0, count // SHARE, body, 0)


def kernel(
    EP,
    Z,
    mix_x,
    mix_gain_h,
    value_w,
    inner_w,
    outer_w,
    taps_h,
    mix_w,
    moe_x,
    moe_gain_h,
    router_g_h,
    router_e_h,
    routes_h,
    gate_w,
    up_w,
    down_w,
    out,
    mix_gain,
    taps,
    moe_gain,
    router_g,
    router_e,
    routes,
    raw_m,
    raw_e,
    norm_m,
    norm_e,
    gu_w,
    dn_w,
    proj_w,
    mixw,
    send,
    recv,
    acc,
    rs_send,
    rs_recv,
    mix_send,
    mix_recv,
    halo_out,
    halo_in,
    gated,
    outer_p,
    conv,
    conv_all,
    mix_part,
    comb_w,
    ret_send,
    ret_recv,
    comb,
    comb_in,
    out_v,
    load_sem,
    tok_sem,
    small_sem,
    swap_send,
    swap_recv,
    disp_send,
    disp_recv,
    credit,
    hop_send,
    hop_recv,
    mixhop_send,
    mixhop_recv,
    halo_sem,
    conv_sem,
    back_send,
    back_recv,
    last_send,
    last_recv,
    out_sem,
):
    tokens, width = raw_m.shape
    C = value_w.shape[1]
    F = gate_w.shape[1]
    half = EP // 2
    rows = half * 2 * CAP
    piece = width // PIECES
    hops = Z // 2
    fine = piece // FINE
    parts = PIECES * FINE

    e = lax.axis_index("ep")
    tp = lax.axis_index("tp")
    z, c = tp // 2, lax.rem(tp, 2)
    ep_odd = lax.rem(e, 2)
    slot = e // 2
    partner = (e, z * 2 + 1 - c)

    def to_expert(i):
        return (2 * i + c, z * 2 + 1 - ep_odd)

    def to_source(i):
        return (2 * i + 1 - c, z * 2 + ep_odd)

    def beside(step):
        return (e, lax.rem(z + step + Z, Z) * 2 + c)

    def remote(src, dst, ssem, rsem, device):
        return pltpu.make_async_remote_copy(
            src_ref=src, dst_ref=dst, send_sem=ssem, recv_sem=rsem, device_id=device, device_id_type=MESH
        )

    home = 2 * SHARE

    def home_of(s):
        k = (s + 1) // 2
        sign = 2 * lax.rem(s, 2) - 1
        return lax.rem(z + jnp.where(s == 0, hops, sign * (hops - k)) + Z, Z)

    def token_load(s):
        span = pl.ds(pl.multiple_of(home_of(s) * home, home), home)
        return pltpu.make_async_copy(moe_x.at[span], raw_e.at[span], tok_sem.at[s])

    smalls = [
        pltpu.make_async_copy(src, dst, small_sem.at[n])
        for n, (src, dst) in enumerate(
            [
                (routes_h, routes),
                (moe_gain_h, moe_gain),
                (mix_gain_h, mix_gain),
                (taps_h, taps),
                (router_g_h, router_g),
                (router_e_h, router_e),
            ]
        )
    ]
    loads = [
        pltpu.make_async_copy(src, dst, load_sem.at[n])
        for n, (src, dst) in enumerate(
            [
                (mix_x, raw_m),
                (value_w, proj_w.at[:, 0:C]),
                (inner_w, proj_w.at[:, C : 2 * C]),
                (outer_w, proj_w.at[:, 2 * C : 3 * C]),
                (mix_w, mixw.at[0:C]),
                (gate_w, gu_w.at[:, 0:F]),
                (up_w, gu_w.at[:, 2 * F : 3 * F]),
                (down_w, dn_w.at[0:F]),
            ]
        )
    ]
    smalls[0].start()
    token_load(0).start()
    smalls[1].start()
    barrier = pltpu.get_barrier_semaphore()
    greet = [to_expert(i) for i in range(half)] + [to_source(i) for i in range(half)]
    greet += [beside(1), beside(-1)]
    greet += [(lax.rem(e + 1, EP), tp), (lax.rem(e + EP - 1, EP), tp)]
    for device in greet:
        pl.semaphore_signal(barrier, inc=1, device_id=device, device_id_type=MESH)
    smalls[2].start()
    for copy in loads[0:4]:
        copy.start()

    def load_tokens(s, carry):
        token_load(s).start()
        return carry

    lax.fori_loop(1, Z, load_tokens, 0)
    for copy in loads[4:] + smalls[3:]:
        copy.start()

    row = lax.broadcasted_iota(jnp.int32, (rows, home), 0)
    tok = lax.broadcasted_iota(jnp.int32, (rows, home), 1)
    expert_of = (2 * (row >> 3) + c).astype(F32)
    slot_of = (row & 3).astype(F32)
    in_block = (tok >> 4) == ((row >> 2) & 1)
    bef_r = lax.broadcasted_iota(jnp.int32, (home, home), 0)
    bef_c = lax.broadcasted_iota(jnp.int32, (home, home), 1)
    before = ((bef_r < bef_c) & ((bef_r >> 4) == (bef_c >> 4))).astype(F32).astype(BF16)
    pick_r = lax.broadcasted_iota(jnp.int32, (tokens, home), 0)
    pick_c = lax.broadcasted_iota(jnp.int32, (tokens, home), 1)
    smalls[0].wait()
    routes_b = routes[...].astype(F32).astype(BF16)

    def routed(zh):
        pick = (pick_r == pick_c + zh * home).astype(F32).astype(BF16)
        named = jnp.dot(routes_b, pick, preferred_element_type=F32)
        h0, h1 = named[0:1, :], named[1:2, :]
        is0, is1 = h0 == expert_of, h1 == expert_of
        rank = jnp.dot((is0 | is1).astype(F32).astype(BF16), before, preferred_element_type=F32)
        at = (rank == slot_of) & in_block
        return h0, h1, at & is0, at & is1

    def dispatch(s):
        y, x = e // SIDE, lax.rem(e, SIDE)
        odd = lax.rem(c + x, 2)
        for dy in (2, 1, 3, 0):
            for n in (0, 1):
                dx = 2 - 2 * n + odd * (4 * n - 1)
                i = (lax.rem(y + dy, SIDE) * SIDE + lax.rem(x + dx, SIDE)) // 2
                remote(send.at[s, i], recv.at[s, slot], disp_send.at[s], disp_recv.at[s], to_expert(i)).start()

    def place(s):
        zh = home_of(s)
        _, _, at0, at1 = routed(zh)
        chosen = (at0 | at1).astype(F32).astype(BF16)
        start = pl.multiple_of(zh * home, home)
        token_load(s).wait()
        rms_rows(raw_e, moe_gain[...], norm_e, start, home)
        for n in range(width // WIDE):
            cols = slice(n * WIDE, (n + 1) * WIDE)
            placed = jnp.dot(chosen, norm_e[pl.ds(start, home), cols], preferred_element_type=F32)
            send[s, :, :, cols] = placed.reshape(half, 2 * CAP, WIDE).astype(BF16)

    swaps = [
        remote(src, dst, swap_send.at[n], swap_recv.at[n], partner)
        for n, (src, dst) in enumerate(
            [
                (gate_w, gu_w.at[:, F : 2 * F]),
                (up_w, gu_w.at[:, 3 * F : 4 * F]),
                (mix_w, mixw.at[C : 2 * C]),
                (down_w, dn_w.at[F : 2 * F]),
            ]
        )
    ]
    halo = remote(halo_out, halo_in, halo_sem.at[0], halo_sem.at[1], (lax.rem(e + 1, EP), tp))
    conv_swap = remote(conv.at[1 - c], conv_all.at[:, C : 2 * C], conv_sem.at[0], conv_sem.at[1], partner)

    def mixer_tail():
        smalls[2].wait()
        loads[0].wait()
        rms_rows(raw_m, mix_gain[...], norm_m, tokens - SHARE, SHARE)
        for n in (1, 2):
            loads[n].wait()
        tail = jnp.dot(norm_m[tokens - SHARE :, :], proj_w[:, 0 : 2 * C], preferred_element_type=F32)
        halo_out[...] = (tail[:, C:] * tail[:, 0:C]).astype(BF16)

    def mixer_proj():
        rms_rows(raw_m, mix_gain[...], norm_m, 0, tokens - SHARE)
        loads[3].wait()
        proj = jnp.dot(norm_m[...], proj_w[...], preferred_element_type=F32)
        gated_in = (proj[:, C : 2 * C] * proj[:, 0:C]).astype(BF16)
        outer_p[...] = proj[:, 2 * C : 3 * C]
        gated[pl.ds(SHARE, tokens), :] = gated_in.astype(F32)

    def mixer_conv():
        halo.wait()
        smalls[3].wait()
        gated[0:SHARE, :] = jnp.where(e > 0, halo_in[...].astype(F32), 0.0)
        mixed = taps[0:1, :] * gated[pl.ds(SHARE - 2, tokens), :]
        mixed = mixed + taps[1:2, :] * gated[pl.ds(SHARE - 1, tokens), :]
        mixed = mixed + taps[2:3, :] * gated[pl.ds(SHARE, tokens), :]
        conv_out = (outer_p[...] * mixed).astype(BF16).reshape(Z, 2, SHARE, C)
        conv[0] = conv_out[:, 0].reshape(Z * SHARE, C)
        conv[1] = conv_out[:, 1].reshape(Z * SHARE, C)
        conv_swap.start()
        swaps[1].start()
        swaps[3].start()
        conv_all[:, 0:C] = conv[c]

    def mix_hop(direction, k):
        return remote(
            mix_send.at[direction, k],
            mix_recv.at[direction, k],
            mixhop_send.at[direction, k],
            mixhop_recv.at[direction, k],
            beside(2 * direction - 1),
        )

    def mixer_hop(direction, k):
        zh = lax.rem(z + (2 * direction - 1) * (hops - k) + Z, Z)
        came = k > 1 or (k == 1 and direction == 1)
        if came:
            mix_hop(direction, k - 1).wait_recv()
        for part in (0, 1):
            total = mix_part[zh, :, part * (width // 2) : (part + 1) * (width // 2)]
            if came:
                total = total + mix_recv[direction, k - 1, part].astype(F32)
            mix_send[direction, k, part] = total.astype(BF16)
        mix_hop(direction, k).start()

    mix_write = pltpu.make_async_copy(out_v.at[0], out.at[0], out_sem.at[parts])

    def mixer_end():
        for direction in (1, 0):
            mix_hop(direction, hops - 1).wait_recv()
        for part in (0, 1):
            cols = slice(part * (width // 2), (part + 1) * (width // 2))
            total = mix_part[z, :, cols] + mix_recv[1, hops - 1, part].astype(F32)
            out_v[0, :, cols] = (total + mix_recv[0, hops - 1, part].astype(F32)).astype(BF16)
        mix_write.start()

    def mixer_down():
        loads[4].wait()
        swaps[2].wait_recv()
        conv_swap.wait()

        for n in range(width // WIDE):
            cols = slice(n * WIDE, (n + 1) * WIDE)
            part = jnp.dot(conv_all[...], mixw[:, cols], preferred_element_type=F32)
            mix_part[:, :, cols] = part.reshape(Z, SHARE, WIDE)
        mixer_hop(1, 0)
        mixer_hop(0, 1)

    def weigh():
        smalls[4].wait()
        smalls[5].wait()
        h0, h1, at0, at1 = routed(z)
        own_normed = norm_e[pl.ds(pl.multiple_of(z * home, home), home), :]
        contract_last = (((1,), (1,)), ((), ()))
        group_logit = lax.dot_general(router_g[...], own_normed, contract_last, preferred_element_type=F32)
        expert_logit = lax.dot_general(router_e[...], own_normed, contract_last, preferred_element_type=F32)
        group_exp = jnp.exp(group_logit)
        first_of = (lax.broadcasted_iota(jnp.int32, group_exp.shape, 0) * EPG).astype(F32)
        in_group = (h0 >= first_of) & (h0 < first_of + EPG)
        gate = jnp.sum(jnp.where(in_group, group_exp, 0.0), axis=0, keepdims=True) / jnp.sum(
            group_exp, axis=0, keepdims=True
        )
        number = lax.broadcasted_iota(jnp.int32, expert_logit.shape, 0).astype(F32)
        chosen0 = jnp.exp(jnp.sum(jnp.where(number == h0, expert_logit, 0.0), axis=0, keepdims=True))
        chosen1 = jnp.exp(jnp.sum(jnp.where(number == h1, expert_logit, 0.0), axis=0, keepdims=True))
        both = chosen0 + chosen1
        weight = jnp.where(at0, gate * chosen0 / both, 0.0) + jnp.where(at1, gate * chosen1 / both, 0.0)
        weight = weight.T
        high = weight.astype(BF16)
        comb_w[0:home, :] = high
        comb_w[home : 2 * home, :] = (weight - high.astype(F32)).astype(BF16)

    def hop(direction, k, j, h):
        cols = slice(h * fine, (h + 1) * fine)
        return remote(
            rs_send.at[direction, k, j, :, cols],
            rs_recv.at[direction, k, j, :, cols],
            hop_send.at[direction, k, j, h],
            hop_recv.at[direction, k, j, h],
            beside(2 * direction - 1),
        )

    def give_back(p, i):
        return remote(ret_send.at[p, i], ret_recv.at[p, slot], back_send.at[p], back_recv.at[p], to_source(i))

    def stage(s, carry):
        for direction, k, when in MIX_HOPS:

            @pl.when(s == when)
            def _():
                mixer_hop(direction, k)

        @pl.when((s > 0) & (s - 1 + AHEAD < Z))
        def _():
            place(s - 1 + AHEAD)
            pl.semaphore_wait(credit.at[s - 1], half)
            dispatch(s - 1 + AHEAD)

        @pl.when(s == 0)
        def _():
            for n in (5, 6, 7):
                loads[n].wait()
            for n in (0, 1, 3):
                swaps[n].wait_recv()

        @pl.when(s == Z - 1)
        def _():
            mixer_end()

        @pl.when(s == Z + 1 - AHEAD)
        def _():
            weigh()

        arrived = remote(send.at[s], recv.at[s], disp_send.at[s], disp_recv.at[s], partner)
        arrived.wait_recv()

        @pl.when(s + AHEAD < Z)
        def _():
            for i in range(half):
                pl.semaphore_signal(credit.at[s], inc=1, device_id=to_source(i), device_id_type=MESH)

        x = recv[s].reshape(rows, width)
        gate_up = jnp.dot(x, gu_w[...], preferred_element_type=F32)
        g, u = gate_up[:, 0 : 2 * F], gate_up[:, 2 * F :]
        hidden = (g / (1.0 + jnp.exp(-g)) * u).astype(BF16)
        direction = lax.rem(s, 2)
        k = (s + 1) // 2
        for j in range(PIECES):
            cols = slice(j * piece, (j + 1) * piece)
            side = 1 if j < PIECES // 2 else 0
            acc[...] = jnp.dot(hidden, dn_w[:, cols], preferred_element_type=F32)

            @pl.when(s == 0)
            def _():
                rs_send[side, 0, j] = acc[...].astype(BF16)
                for h in range(FINE):
                    hop(side, 0, j, h).start()

            @pl.when((s > 0) & (s < Z - 1))
            def _():
                @pl.when((k == 1) & (direction == side))
                def _():
                    for h in range(FINE):
                        hop(side, 0, j, h).wait_recv()
                    acc[...] += rs_recv[side, 0, j].astype(F32)

                @pl.when(k > 1)
                def _():
                    for h in range(FINE):
                        hop(direction, k - 1, j, h).wait_recv()
                    acc[...] += rs_recv[direction, k - 1, j].astype(F32)

                rs_send[direction, k, j] = acc[...].astype(BF16)
                for h in range(FINE):
                    hop(direction, k, j, h).start()

            @pl.when(s == Z - 1)
            def _():
                for h in range(FINE):
                    span = slice(h * fine, (h + 1) * fine)
                    for way in (1, 0):
                        hop(way, hops - 1, j, h).wait_recv()
                    total = acc[:, span] + rs_recv[1, hops - 1, j, :, span].astype(F32)
                    total = total + rs_recv[0, hops - 1, j, :, span].astype(F32)
                    p = j * FINE + h
                    ret_send[p] = total.astype(BF16).reshape(half, 2 * CAP, fine)
                    for i in range(half):
                        give_back(p, i).start()

        return carry

    smalls[1].wait()
    place(jnp.int32(0))
    mixer_tail()
    pl.semaphore_wait(barrier, len(greet))
    halo.start()
    dispatch(jnp.int32(0))
    for n in (2, 0):
        swaps[n].start()
    mixer_proj()
    mixer_conv()
    place(jnp.int32(1))
    dispatch(jnp.int32(1))
    mixer_down()

    def place_early(s, carry):
        place(s)
        dispatch(s)
        return carry

    lax.fori_loop(2, AHEAD, place_early, 0)
    lax.fori_loop(0, Z, stage, 0)

    def last(p):
        return remote(comb.at[p, 1 - c], comb_in.at[p], last_send.at[p], last_recv.at[p], partner)

    def returned(p):
        return remote(ret_send.at[p], ret_recv.at[p], back_send.at[p], back_recv.at[p], partner)

    def finish(p):
        last(p).wait_recv()
        cols = slice(p * fine, (p + 1) * fine)
        out_v[1, :, cols] = (comb[p, c] + comb_in[p]).astype(BF16)
        write(p).start()

    def write(p):
        cols = slice(p * fine, (p + 1) * fine)
        return pltpu.make_async_copy(out_v.at[1, :, cols], out.at[1, :, cols], out_sem.at[p])

    for p in range(parts):
        returned(p).wait_recv()
        summed = jnp.dot(comb_w[...], ret_recv[p].reshape(rows, fine), preferred_element_type=F32)
        comb[p] = (summed[0:home] + summed[home:]).reshape(2, SHARE, fine)
        last(p).start()
        if p > 1:
            finish(p - 2)
    for p in range(parts - 2, parts):
        finish(p)

    for copy in swaps:
        copy.wait_send()
    for k in range(hops):
        for direction in (0, 1):
            if k or direction:
                mix_hop(direction, k).wait_send()
    for s in range(Z):
        remote(send.at[s], recv.at[s], disp_send.at[s], disp_recv.at[s], partner).wait_send()
    for j in range(PIECES):
        for h in range(FINE):
            hop(1 if j < PIECES // 2 else 0, 0, j, h).wait_send()
            for k in range(1, hops):
                for direction in (0, 1):
                    hop(direction, k, j, h).wait_send()
    for p in range(parts):
        returned(p).wait_send()
        last(p).wait_send()
        write(p).wait()
    mix_write.wait()


def solution(mesh):
    EP, TP = mesh.shape["ep"], mesh.shape["tp"]
    Z = TP // 2

    def local(
        mix_tokens,
        mix_gain,
        value_weight,
        inner_weight,
        outer_weight,
        conv_taps,
        mix_weight,
        moe_tokens,
        moe_gain,
        router_group,
        router_expert,
        expert_routes,
        gate_weight,
        up_weight,
        down_weight,
    ):
        tokens, D = mix_tokens.shape
        C = value_weight.shape[1]
        F = gate_weight.shape[2]
        half = EP // 2
        rows = half * 2 * CAP
        piece = D // PIECES
        hops = Z // 2
        fine = piece // FINE
        parts = PIECES * FINE
        hbm = pl.BlockSpec(memory_space=pl.ANY)
        V = pltpu.VMEM
        DMA = pltpu.SemaphoreType.DMA
        both = pl.pallas_call(
            functools.partial(kernel, EP, Z),
            out_shape=jax.ShapeDtypeStruct((2, SHARE, D), BF16),
            in_specs=[hbm] * 15,
            out_specs=hbm,
            scratch_shapes=[
                V((1, D), F32),
                V(conv_taps.shape, F32),
                V((1, D), F32),
                V((router_group.shape[1], D), BF16),
                V((router_expert.shape[1], D), BF16),
                V((2, tokens), jnp.int32),
                V((tokens, D), BF16),
                V((tokens, D), BF16),
                V((tokens, D), BF16),
                V((tokens, D), BF16),
                V((D, 4 * F), BF16),
                V((2 * F, D), BF16),
                V((D, 3 * C), BF16),
                V((2 * C, D), BF16),
                V((Z, half, 2 * CAP, D), BF16),
                V((Z, half, 2 * CAP, D), BF16),
                V((rows, piece), F32),
                V((2, hops, PIECES, rows, piece), BF16),
                V((2, hops, PIECES, rows, piece), BF16),
                V((2, hops, 2, SHARE, D // 2), BF16),
                V((2, hops, 2, SHARE, D // 2), BF16),
                V((SHARE, C), BF16),
                V((SHARE, C), BF16),
                V((SHARE + tokens, C), F32),
                V((tokens, C), F32),
                V((2, Z * SHARE, C), BF16),
                V((Z * SHARE, 2 * C), BF16),
                V((Z, SHARE, D), F32),
                V((4 * SHARE, rows), BF16),
                V((parts, half, 2 * CAP, fine), BF16),
                V((parts, half, 2 * CAP, fine), BF16),
                V((parts, 2, SHARE, fine), F32),
                V((parts, SHARE, fine), F32),
                V((2, SHARE, D), BF16),
                DMA((8,)),
                DMA((Z,)),
                DMA((6,)),
                DMA((4,)),
                DMA((4,)),
                DMA((Z,)),
                DMA((Z,)),
                pltpu.SemaphoreType.REGULAR((Z,)),
                DMA((2, hops, PIECES, FINE)),
                DMA((2, hops, PIECES, FINE)),
                DMA((2, hops)),
                DMA((2, hops)),
                DMA((2,)),
                DMA((2,)),
                DMA((parts,)),
                DMA((parts,)),
                DMA((parts,)),
                DMA((parts,)),
                DMA((parts + 1,)),
            ],
            compiler_params=pltpu.CompilerParams(
                collective_id=0, has_side_effects=True, vmem_limit_bytes=VMEM_MIB * 1024 * 1024
            ),
            name="mixer_and_experts",
        )(
            mix_tokens,
            mix_gain.reshape(1, D),
            value_weight,
            inner_weight,
            outer_weight,
            conv_taps,
            mix_weight,
            moe_tokens,
            moe_gain.reshape(1, D),
            router_group.T,
            router_expert.T,
            expert_routes.T,
            gate_weight.reshape(D, F),
            up_weight.reshape(D, F),
            down_weight.reshape(F, D),
        )
        return both[0], both[1]

    return jax.shard_map(
        local,
        mesh=mesh,
        in_specs=(
            P("ep", None),
            P(),
            P(None, "tp"),
            P(None, "tp"),
            P(None, "tp"),
            P(None, "tp"),
            P("tp", None),
            P("ep", None),
            P(),
            P(),
            P(),
            P("ep", None),
            P("ep", None, "tp"),
            P("ep", None, "tp"),
            P("ep", "tp", None),
        ),
        out_specs=(P(("ep", "tp"), None), P(("ep", "tp"), None)),
        check_vma=False,
    )
```

```python
import functools

import jax
import jax.numpy as jnp
from jax import lax
from jax.experimental import pallas as pl
from jax.experimental.pallas import tpu as pltpu
from jax.sharding import PartitionSpec as P

MESH = pl.DeviceIdType.MESH
F32 = jnp.float32
BF16 = jnp.bfloat16
SHARE = 16
CAP = 4
EPG = 4
EPS = 1e-06
PIECES = 4
WIDE = 2048
UNROLL = 3
FINE = 1
MIX_HOPS = ((0, 2, 0), (1, 1, 0), (0, 3, 2), (1, 2, 2), (1, 3, 5))
VMEM_MIB = 60
SIDE = 4
AHEAD = 3


def rms_rows(raw, gain, out, start, count):
    def body(i, carry):
        rows = pl.ds(pl.multiple_of(start + i * SHARE, SHARE), SHARE)
        values = raw[rows, :].astype(F32)
        inverse = lax.rsqrt(jnp.mean(values * values, axis=-1, keepdims=True) + EPS)
        out[rows, :] = (values * inverse * gain).astype(BF16)
        return carry

    trips = count // SHARE
    lax.fori_loop(0, trips, body, 0, unroll=UNROLL if trips % UNROLL == 0 else 2 if trips % 2 == 0 else 1)


def kernel(
    EP,
    Z,
    mix_x,
    mix_gain_h,
    value_w,
    inner_w,
    outer_w,
    taps_h,
    mix_w,
    moe_x,
    moe_gain_h,
    router_g_h,
    router_e_h,
    routes_h,
    gate_w,
    up_w,
    down_w,
    out,
    mix_gain,
    taps,
    moe_gain,
    router_g,
    router_e,
    routes,
    raw_m,
    raw_e,
    norm_m,
    norm_e,
    gu_w,
    dn_w,
    proj_w,
    mixw,
    send,
    recv,
    acc,
    rs_send,
    rs_recv,
    mix_send,
    mix_recv,
    halo_out,
    halo_in,
    gated,
    outer_p,
    conv,
    conv_all,
    mix_part,
    comb_w,
    ret_send,
    ret_recv,
    comb,
    comb_in,
    out_v,
    load_sem,
    tok_sem,
    small_sem,
    swap_send,
    swap_recv,
    disp_send,
    disp_recv,
    credit,
    hop_send,
    hop_recv,
    mixhop_send,
    mixhop_recv,
    halo_sem,
    conv_sem,
    back_send,
    back_recv,
    last_send,
    last_recv,
    out_sem,
):
    tokens, width = raw_m.shape
    C = value_w.shape[1]
    F = gate_w.shape[1]
    half = EP // 2
    rows = half * 2 * CAP
    piece = width // PIECES
    hops = Z // 2
    fine = piece // FINE
    parts = PIECES * FINE

    e = lax.axis_index("ep")
    tp = lax.axis_index("tp")
    z, c = tp // 2, lax.rem(tp, 2)
    ep_odd = lax.rem(e, 2)
    slot = e // 2
    partner = (e, z * 2 + 1 - c)

    def to_expert(i):
        return (2 * i + c, z * 2 + 1 - ep_odd)

    def to_source(i):
        return (2 * i + 1 - c, z * 2 + ep_odd)

    def beside(step):
        return (e, lax.rem(z + step + Z, Z) * 2 + c)

    def remote(src, dst, ssem, rsem, device):
        return pltpu.make_async_remote_copy(
            src_ref=src, dst_ref=dst, send_sem=ssem, recv_sem=rsem, device_id=device, device_id_type=MESH
        )

    home = 2 * SHARE

    def home_of(s):
        k = (s + 1) // 2
        sign = 2 * lax.rem(s, 2) - 1
        return lax.rem(z + jnp.where(s == 0, hops, sign * (hops - k)) + Z, Z)

    def token_load(s):
        span = pl.ds(pl.multiple_of(home_of(s) * home, home), home)
        return pltpu.make_async_copy(moe_x.at[span], raw_e.at[span], tok_sem.at[s])

    smalls = [
        pltpu.make_async_copy(src, dst, small_sem.at[n])
        for n, (src, dst) in enumerate(
            [
                (routes_h, routes),
                (moe_gain_h, moe_gain),
                (mix_gain_h, mix_gain),
                (taps_h, taps),
                (router_g_h, router_g),
                (router_e_h, router_e),
            ]
        )
    ]
    loads = [
        pltpu.make_async_copy(src, dst, load_sem.at[n])
        for n, (src, dst) in enumerate(
            [
                (mix_x, raw_m),
                (value_w, proj_w.at[:, 0:C]),
                (inner_w, proj_w.at[:, C : 2 * C]),
                (outer_w, proj_w.at[:, 2 * C : 3 * C]),
                (mix_w, mixw.at[0:C]),
                (gate_w, gu_w.at[:, 0:F]),
                (up_w, gu_w.at[:, 2 * F : 3 * F]),
                (down_w, dn_w.at[0:F]),
            ]
        )
    ]
    smalls[0].start()
    token_load(0).start()
    smalls[1].start()
    barrier = pltpu.get_barrier_semaphore()
    greet = [to_expert(i) for i in range(half)] + [to_source(i) for i in range(half)]
    greet += [beside(1), beside(-1)]
    greet += [(lax.rem(e + 1, EP), tp), (lax.rem(e + EP - 1, EP), tp)]
    for device in greet:
        pl.semaphore_signal(barrier, inc=1, device_id=device, device_id_type=MESH)
    smalls[2].start()
    for copy in loads[0:4]:
        copy.start()

    def load_tokens(s, carry):
        token_load(s).start()
        return carry

    lax.fori_loop(1, Z, load_tokens, 0)
    for copy in loads[4:] + smalls[3:]:
        copy.start()

    row = lax.broadcasted_iota(jnp.int32, (rows, home), 0)
    tok = lax.broadcasted_iota(jnp.int32, (rows, home), 1)
    expert_of = (2 * (row >> 3) + c).astype(F32)
    slot_of = (row & 3).astype(F32)
    in_block = (tok >> 4) == ((row >> 2) & 1)
    bef_r = lax.broadcasted_iota(jnp.int32, (home, home), 0)
    bef_c = lax.broadcasted_iota(jnp.int32, (home, home), 1)
    before = ((bef_r < bef_c) & ((bef_r >> 4) == (bef_c >> 4))).astype(F32).astype(BF16)
    pick_r = lax.broadcasted_iota(jnp.int32, (tokens, home), 0)
    pick_c = lax.broadcasted_iota(jnp.int32, (tokens, home), 1)
    smalls[0].wait()
    routes_b = routes[...].astype(F32).astype(BF16)

    def routed(zh):
        pick = (pick_r == pick_c + zh * home).astype(F32).astype(BF16)
        named = jnp.dot(routes_b, pick, preferred_element_type=F32)
        h0, h1 = named[0:1, :], named[1:2, :]
        is0, is1 = h0 == expert_of, h1 == expert_of
        rank = jnp.dot((is0 | is1).astype(F32).astype(BF16), before, preferred_element_type=F32)
        at = (rank == slot_of) & in_block
        return h0, h1, at & is0, at & is1

    def dispatch(s):
        y, x = e // SIDE, lax.rem(e, SIDE)
        odd = lax.rem(c + x, 2)
        for dy in (2, 1, 3, 0):
            for n in (0, 1):
                dx = 2 - 2 * n + odd * (4 * n - 1)
                i = (lax.rem(y + dy, SIDE) * SIDE + lax.rem(x + dx, SIDE)) // 2
                remote(send.at[s, i], recv.at[s, slot], disp_send.at[0], disp_recv.at[s], to_expert(i)).start()

    def place(s):
        zh = home_of(s)
        _, _, at0, at1 = routed(zh)
        chosen = (at0 | at1).astype(F32).astype(BF16)
        start = pl.multiple_of(zh * home, home)
        token_load(s).wait()
        rms_rows(raw_e, moe_gain[...], norm_e, start, home)
        for n in range(width // WIDE):
            cols = slice(n * WIDE, (n + 1) * WIDE)
            placed = jnp.dot(chosen, norm_e[pl.ds(start, home), cols], preferred_element_type=F32)
            send[s, :, :, cols] = placed.reshape(half, 2 * CAP, WIDE).astype(BF16)

    swaps = [
        remote(src, dst, swap_send.at[n], swap_recv.at[n], partner)
        for n, (src, dst) in enumerate(
            [
                (gate_w, gu_w.at[:, F : 2 * F]),
                (up_w, gu_w.at[:, 3 * F : 4 * F]),
                (mix_w, mixw.at[C : 2 * C]),
                (down_w, dn_w.at[F : 2 * F]),
            ]
        )
    ]
    halo = remote(halo_out, halo_in, halo_sem.at[0], halo_sem.at[1], (lax.rem(e + 1, EP), tp))
    conv_swap = remote(conv.at[1 - c], conv_all.at[:, C : 2 * C], conv_sem.at[0], conv_sem.at[1], partner)

    def mixer_tail():
        smalls[2].wait()
        loads[0].wait()
        rms_rows(raw_m, mix_gain[...], norm_m, tokens - SHARE, SHARE)
        for n in (1, 2):
            loads[n].wait()
        tail = jnp.dot(norm_m[tokens - SHARE :, :], proj_w[:, 0 : 2 * C], preferred_element_type=F32)
        halo_out[...] = (tail[:, C:] * tail[:, 0:C]).astype(BF16)

    def mixer_proj():
        rms_rows(raw_m, mix_gain[...], norm_m, 0, tokens - SHARE)
        loads[3].wait()
        proj = jnp.dot(norm_m[...], proj_w[...], preferred_element_type=F32)
        gated_in = (proj[:, C : 2 * C] * proj[:, 0:C]).astype(BF16)
        outer_p[...] = proj[:, 2 * C : 3 * C]
        gated[pl.ds(SHARE, tokens), :] = gated_in.astype(F32)

    def mixer_conv():
        halo.wait()
        smalls[3].wait()
        gated[0:SHARE, :] = jnp.where(e > 0, halo_in[...].astype(F32), 0.0)
        mixed = taps[0:1, :] * gated[pl.ds(SHARE - 2, tokens), :]
        mixed = mixed + taps[1:2, :] * gated[pl.ds(SHARE - 1, tokens), :]
        mixed = mixed + taps[2:3, :] * gated[pl.ds(SHARE, tokens), :]
        conv_out = (outer_p[...] * mixed).astype(BF16).reshape(Z, 2, SHARE, C)
        conv[0] = conv_out[:, 0].reshape(Z * SHARE, C)
        conv[1] = conv_out[:, 1].reshape(Z * SHARE, C)
        conv_swap.start()
        swaps[1].start()
        swaps[3].start()
        conv_all[:, 0:C] = conv[c]

    def mix_hop(direction, k, part):
        return remote(
            mix_send.at[direction, k, part],
            mix_recv.at[direction, k, part],
            mixhop_send.at[direction, min(k, 1)],
            mixhop_recv.at[direction, k, part],
            beside(2 * direction - 1),
        )

    def mixer_hop(direction, k):
        zh = lax.rem(z + (2 * direction - 1) * (hops - k) + Z, Z)
        for part in (0, 1):
            total = mix_part[zh, :, part * (width // 2) : (part + 1) * (width // 2)]
            if k > 1 or (k == 1 and direction == 1):
                mix_hop(direction, k - 1, part).wait_recv()
                total = total + mix_recv[direction, k - 1, part].astype(F32)
            mix_send[direction, k, part] = total.astype(BF16)
            mix_hop(direction, k, part).start()

    mix_write = pltpu.make_async_copy(out_v.at[0], out.at[0], out_sem.at[0])

    def mixer_end():
        for direction in (1, 0):
            for part in (0, 1):
                mix_hop(direction, hops - 1, part).wait_recv()
        for part in (0, 1):
            cols = slice(part * (width // 2), (part + 1) * (width // 2))
            total = mix_part[z, :, cols] + mix_recv[1, hops - 1, part].astype(F32)
            out_v[0, :, cols] = (total + mix_recv[0, hops - 1, part].astype(F32)).astype(BF16)
        mix_write.start()

    def mixer_down():
        loads[4].wait()
        swaps[2].wait_recv()
        conv_swap.wait()

        for n in range(width // WIDE):
            cols = slice(n * WIDE, (n + 1) * WIDE)
            part = jnp.dot(conv_all[...], mixw[:, cols], preferred_element_type=F32)
            mix_part[:, :, cols] = part.reshape(Z, SHARE, WIDE)
        mixer_hop(1, 0)
        mixer_hop(0, 1)

    def weigh():
        smalls[4].wait()
        smalls[5].wait()
        h0, h1, at0, at1 = routed(z)
        own_normed = norm_e[pl.ds(pl.multiple_of(z * home, home), home), :]
        contract_last = (((1,), (1,)), ((), ()))
        group_logit = lax.dot_general(router_g[...], own_normed, contract_last, preferred_element_type=F32)
        expert_logit = lax.dot_general(router_e[...], own_normed, contract_last, preferred_element_type=F32)
        group_exp = jnp.exp(group_logit)
        first_of = (lax.broadcasted_iota(jnp.int32, group_exp.shape, 0) * EPG).astype(F32)
        in_group = (h0 >= first_of) & (h0 < first_of + EPG)
        gate = jnp.sum(jnp.where(in_group, group_exp, 0.0), axis=0, keepdims=True) / jnp.sum(
            group_exp, axis=0, keepdims=True
        )
        number = lax.broadcasted_iota(jnp.int32, expert_logit.shape, 0).astype(F32)
        chosen0 = jnp.exp(jnp.sum(jnp.where(number == h0, expert_logit, 0.0), axis=0, keepdims=True))
        chosen1 = jnp.exp(jnp.sum(jnp.where(number == h1, expert_logit, 0.0), axis=0, keepdims=True))
        both = chosen0 + chosen1
        weight = jnp.where(at0, gate * chosen0 / both, 0.0) + jnp.where(at1, gate * chosen1 / both, 0.0)
        weight = weight.T
        high = weight.astype(BF16)
        comb_w[0:home, :] = high
        comb_w[home : 2 * home, :] = (weight - high.astype(F32)).astype(BF16)

    def hop(direction, k, j, h):
        cols = slice(h * fine, (h + 1) * fine)
        return remote(
            rs_send.at[direction, k, j, :, cols],
            rs_recv.at[direction, k, j, :, cols],
            hop_send.at[direction, jnp.minimum(k, 1)],
            hop_recv.at[direction, k, j, h],
            beside(2 * direction - 1),
        )

    def give_back(p, i):
        return remote(ret_send.at[p, i], ret_recv.at[p, slot], back_send.at[0], back_recv.at[p], to_source(i))

    def stage(s, carry):
        for direction, k, when in MIX_HOPS:

            @pl.when(s == when)
            def _():
                mixer_hop(direction, k)

        @pl.when((s > 0) & (s - 1 + AHEAD < Z))
        def _():
            place(s - 1 + AHEAD)
            pl.semaphore_wait(credit.at[s - 1], half)
            dispatch(s - 1 + AHEAD)

        @pl.when(s == 0)
        def _():
            for n in (5, 6, 7):
                loads[n].wait()
            for n in (0, 1, 3):
                swaps[n].wait_recv()

        @pl.when(s == Z - 1)
        def _():
            mixer_end()

        @pl.when(s == Z + 1 - AHEAD)
        def _():
            weigh()

        arrived = remote(send.at[s], recv.at[s], disp_send.at[0], disp_recv.at[s], partner)
        arrived.wait_recv()

        @pl.when(s + AHEAD < Z)
        def _():
            for i in range(half):
                pl.semaphore_signal(credit.at[s], inc=1, device_id=to_source(i), device_id_type=MESH)

        x = recv[s].reshape(rows, width)
        gate_up = jnp.dot(x, gu_w[...], preferred_element_type=F32)
        g, u = gate_up[:, 0 : 2 * F], gate_up[:, 2 * F :]
        hidden = (g / (1.0 + jnp.exp(-g)) * u).astype(BF16)
        direction = lax.rem(s, 2)
        k = (s + 1) // 2
        for j in range(PIECES):
            cols = slice(j * piece, (j + 1) * piece)
            side = 1 if j < PIECES // 2 else 0
            acc[...] = jnp.dot(hidden, dn_w[:, cols], preferred_element_type=F32)

            @pl.when(s == 0)
            def _():
                rs_send[side, 0, j] = acc[...].astype(BF16)
                for h in range(FINE):
                    hop(side, 0, j, h).start()

            @pl.when((s > 0) & (s < Z - 1))
            def _():
                @pl.when((k == 1) & (direction == side))
                def _():
                    for h in range(FINE):
                        hop(side, 0, j, h).wait_recv()
                    acc[...] += rs_recv[side, 0, j].astype(F32)

                @pl.when(k > 1)
                def _():
                    for h in range(FINE):
                        hop(direction, k - 1, j, h).wait_recv()
                    acc[...] += rs_recv[direction, k - 1, j].astype(F32)

                rs_send[direction, k, j] = acc[...].astype(BF16)
                for h in range(FINE):
                    hop(direction, k, j, h).start()

            @pl.when(s == Z - 1)
            def _():
                for h in range(FINE):
                    span = slice(h * fine, (h + 1) * fine)
                    for way in (1, 0):
                        hop(way, hops - 1, j, h).wait_recv()
                    total = acc[:, span] + rs_recv[1, hops - 1, j, :, span].astype(F32)
                    total = total + rs_recv[0, hops - 1, j, :, span].astype(F32)
                    p = j * FINE + h
                    ret_send[p] = total.astype(BF16).reshape(half, 2 * CAP, fine)
                    for i in range(half):
                        give_back(p, i).start()

        return carry

    smalls[1].wait()
    place(jnp.int32(0))
    mixer_tail()
    pl.semaphore_wait(barrier, len(greet))
    halo.start()
    dispatch(jnp.int32(0))
    for n in (2, 0):
        swaps[n].start()
    mixer_proj()
    mixer_conv()
    place(jnp.int32(1))
    dispatch(jnp.int32(1))
    mixer_down()

    def place_early(s, carry):
        place(s)
        dispatch(s)
        return carry

    lax.fori_loop(2, AHEAD, place_early, 0)
    lax.fori_loop(0, Z, stage, 0)

    def last(p):
        return remote(comb.at[1 - c, p], comb_in.at[p], last_send.at[0], last_recv.at[p], partner)

    def returned(p):
        return remote(ret_send.at[p], ret_recv.at[p], back_send.at[0], back_recv.at[p], partner)

    def finish(p):
        last(p).wait_recv()
        cols = slice(p * fine, (p + 1) * fine)
        out_v[1, :, cols] = (comb[c, p] + comb_in[p]).astype(BF16)
        write(p).start()

    def write(p):
        cols = slice(p * fine, (p + 1) * fine)
        return pltpu.make_async_copy(out_v.at[1, :, cols], out.at[1, :, cols], out_sem.at[1])

    for p in range(parts):
        returned(p).wait_recv()
        summed = jnp.dot(comb_w[...], ret_recv[p].reshape(rows, fine), preferred_element_type=F32)
        summed = summed[0:home] + summed[home:]
        comb[0, p] = summed[0:SHARE]
        comb[1, p] = summed[SHARE:]
        last(p).start()
        if p > 1:
            finish(p - 2)
    for p in range(parts - 2, parts):
        finish(p)

    for copy in swaps:
        copy.wait_send()
    remote(mix_send.at[1, 0], mix_recv.at[1, 0], mixhop_send.at[1, 0], mixhop_recv.at[1, 0, 0], partner).wait_send()
    remote(send, recv, disp_send.at[0], disp_recv.at[0], partner).wait_send()
    for way in (0, 1):
        later = pl.ds(1, hops - 1)
        near = pl.ds((1 - way) * (PIECES // 2), PIECES // 2)
        remote(
            mix_send.at[way, later], mix_recv.at[way, later], mixhop_send.at[way, 1], mixhop_recv.at[way, 1, 0], partner
        ).wait_send()
        remote(
            rs_send.at[way, 0, near], rs_recv.at[way, 0, near], hop_send.at[way, 0], hop_recv.at[way, 0, 0, 0], partner
        ).wait_send()
        remote(
            rs_send.at[way, later], rs_recv.at[way, later], hop_send.at[way, 1], hop_recv.at[way, 1, 0, 0], partner
        ).wait_send()
    remote(ret_send, ret_recv, back_send.at[0], back_recv.at[0], partner).wait_send()
    remote(comb.at[1 - c], comb_in, last_send.at[0], last_recv.at[0], partner).wait_send()
    pltpu.make_async_copy(out_v.at[1], out.at[1], out_sem.at[1]).wait()
    mix_write.wait()


def solution(mesh):
    EP, TP = mesh.shape["ep"], mesh.shape["tp"]
    Z = TP // 2

    def local(
        mix_tokens,
        mix_gain,
        value_weight,
        inner_weight,
        outer_weight,
        conv_taps,
        mix_weight,
        moe_tokens,
        moe_gain,
        router_group,
        router_expert,
        expert_routes,
        gate_weight,
        up_weight,
        down_weight,
    ):
        tokens, D = mix_tokens.shape
        C = value_weight.shape[1]
        F = gate_weight.shape[2]
        half = EP // 2
        rows = half * 2 * CAP
        piece = D // PIECES
        hops = Z // 2
        fine = piece // FINE
        parts = PIECES * FINE
        hbm = pl.BlockSpec(memory_space=pl.ANY)
        V = pltpu.VMEM
        DMA = pltpu.SemaphoreType.DMA
        both = pl.pallas_call(
            functools.partial(kernel, EP, Z),
            out_shape=jax.ShapeDtypeStruct((2, SHARE, D), BF16),
            in_specs=[hbm] * 15,
            out_specs=hbm,
            scratch_shapes=[
                V((1, D), F32),
                V(conv_taps.shape, F32),
                V((1, D), F32),
                V((router_group.shape[1], D), BF16),
                V((router_expert.shape[1], D), BF16),
                V((2, tokens), jnp.int32),
                V((tokens, D), BF16),
                V((tokens, D), BF16),
                V((tokens, D), BF16),
                V((tokens, D), BF16),
                V((D, 4 * F), BF16),
                V((2 * F, D), BF16),
                V((D, 3 * C), BF16),
                V((2 * C, D), BF16),
                V((Z, half, 2 * CAP, D), BF16),
                V((Z, half, 2 * CAP, D), BF16),
                V((rows, piece), F32),
                V((2, hops, PIECES, rows, piece), BF16),
                V((2, hops, PIECES, rows, piece), BF16),
                V((2, hops, 2, SHARE, D // 2), BF16),
                V((2, hops, 2, SHARE, D // 2), BF16),
                V((SHARE, C), BF16),
                V((SHARE, C), BF16),
                V((SHARE + tokens, C), F32),
                V((tokens, C), F32),
                V((2, Z * SHARE, C), BF16),
                V((Z * SHARE, 2 * C), BF16),
                V((Z, SHARE, D), F32),
                V((4 * SHARE, rows), BF16),
                V((parts, half, 2 * CAP, fine), BF16),
                V((parts, half, 2 * CAP, fine), BF16),
                V((2, parts, SHARE, fine), F32),
                V((parts, SHARE, fine), F32),
                V((2, SHARE, D), BF16),
                DMA((8,)),
                DMA((Z,)),
                DMA((6,)),
                DMA((4,)),
                DMA((4,)),
                DMA((1,)),
                DMA((Z,)),
                pltpu.SemaphoreType.REGULAR((Z,)),
                DMA((2, 2)),
                DMA((2, hops, PIECES, FINE)),
                DMA((2, 2)),
                DMA((2, hops, 2)),
                DMA((2,)),
                DMA((2,)),
                DMA((1,)),
                DMA((parts,)),
                DMA((1,)),
                DMA((parts,)),
                DMA((2,)),
            ],
            compiler_params=pltpu.CompilerParams(
                collective_id=0, has_side_effects=True, vmem_limit_bytes=VMEM_MIB * 1024 * 1024
            ),
            name="mixer_and_experts",
        )(
            mix_tokens,
            mix_gain.reshape(1, D),
            value_weight,
            inner_weight,
            outer_weight,
            conv_taps,
            mix_weight,
            moe_tokens,
            moe_gain.reshape(1, D),
            router_group.T,
            router_expert.T,
            expert_routes.T,
            gate_weight.reshape(D, F),
            up_weight.reshape(D, F),
            down_weight.reshape(F, D),
        )
        return both[0], both[1]

    return jax.shard_map(
        local,
        mesh=mesh,
        in_specs=(
            P("ep", None),
            P(),
            P(None, "tp"),
            P(None, "tp"),
            P(None, "tp"),
            P(None, "tp"),
            P("tp", None),
            P("ep", None),
            P(),
            P(),
            P(),
            P("ep", None),
            P("ep", None, "tp"),
            P("ep", None, "tp"),
            P("ep", "tp", None),
        ),
        out_specs=(P(("ep", "tp"), None), P(("ep", "tp"), None)),
        check_vma=False,
    )
```

```python
import functools

import jax
import jax.numpy as jnp
from jax import lax
from jax.experimental import pallas as pl
from jax.experimental.pallas import tpu as pltpu
from jax.sharding import PartitionSpec as P

MESH = pl.DeviceIdType.MESH
F32 = jnp.float32
BF16 = jnp.bfloat16
SHARE = 16
CAP = 4
EPG = 4
EPS = 1e-06
PIECES = 4
WIDE = 2048
UNROLL = 3
FINE = 1
MIX_HOPS = ((0, 2, 0), (1, 1, 0), (0, 3, 2), (1, 2, 2), (1, 3, 5))
VMEM_MIB = 60
SIDE = 4
AHEAD = 3


def rms_rows(raw, gain, out, start, count):
    def body(i, carry):
        rows = pl.ds(pl.multiple_of(start + i * SHARE, SHARE), SHARE)
        values = raw[rows, :].astype(F32)
        inverse = lax.rsqrt(jnp.mean(values * values, axis=-1, keepdims=True) + EPS)
        out[rows, :] = (values * inverse * gain).astype(BF16)
        return carry

    trips = count // SHARE
    lax.fori_loop(0, trips, body, 0, unroll=UNROLL if trips % UNROLL == 0 else 2 if trips % 2 == 0 else 1)


def kernel(
    EP,
    Z,
    mix_x,
    mix_gain_h,
    value_w,
    inner_w,
    outer_w,
    taps_h,
    mix_w,
    moe_x,
    moe_gain_h,
    router_g_h,
    router_e_h,
    routes_h,
    gate_w,
    up_w,
    down_w,
    out,
    mix_gain,
    taps,
    moe_gain,
    router_g,
    router_e,
    routes,
    raw_m,
    raw_e,
    norm_m,
    norm_e,
    gu_w,
    dn_w,
    proj_w,
    mixw,
    send,
    recv,
    acc,
    rs_send,
    rs_recv,
    mix_send,
    mix_recv,
    halo_out,
    halo_in,
    gated,
    outer_p,
    conv,
    conv_all,
    mix_part,
    comb_w,
    ret_send,
    ret_recv,
    comb,
    comb_in,
    out_v,
    load_sem,
    tok_sem,
    small_sem,
    swap_send,
    swap_recv,
    disp_send,
    disp_recv,
    credit,
    hop_send,
    hop_recv,
    mixhop_send,
    mixhop_recv,
    halo_sem,
    conv_sem,
    back_send,
    back_recv,
    last_send,
    last_recv,
    out_sem,
):
    tokens, width = raw_m.shape
    C = value_w.shape[1]
    F = gate_w.shape[1]
    half = EP // 2
    rows = half * 2 * CAP
    piece = width // PIECES
    hops = Z // 2
    fine = piece // FINE
    parts = PIECES * FINE

    e = lax.axis_index("ep")
    tp = lax.axis_index("tp")
    z, c = tp // 2, lax.rem(tp, 2)
    ep_odd = lax.rem(e, 2)
    slot = e // 2
    partner = (e, z * 2 + 1 - c)

    def to_expert(i):
        return (2 * i + c, z * 2 + 1 - ep_odd)

    def to_source(i):
        return (2 * i + 1 - c, z * 2 + ep_odd)

    def beside(step):
        return (e, lax.rem(z + step + Z, Z) * 2 + c)

    def remote(src, dst, ssem, rsem, device):
        return pltpu.make_async_remote_copy(
            src_ref=src, dst_ref=dst, send_sem=ssem, recv_sem=rsem, device_id=device, device_id_type=MESH
        )

    home = 2 * SHARE

    def home_of(s):
        k = (s + 1) // 2
        sign = 2 * lax.rem(s, 2) - 1
        return lax.rem(z + jnp.where(s == 0, hops, sign * (hops - k)) + Z, Z)

    def token_load(s):
        span = pl.ds(pl.multiple_of(home_of(s) * home, home), home)
        return pltpu.make_async_copy(moe_x.at[span], raw_e.at[span], tok_sem.at[s])

    smalls = [
        pltpu.make_async_copy(src, dst, small_sem.at[n])
        for n, (src, dst) in enumerate(
            [
                (routes_h, routes),
                (moe_gain_h, moe_gain),
                (mix_gain_h, mix_gain),
                (taps_h, taps),
                (router_g_h, router_g),
                (router_e_h, router_e),
            ]
        )
    ]
    loads = [
        pltpu.make_async_copy(src, dst, load_sem.at[n])
        for n, (src, dst) in enumerate(
            [
                (mix_x, raw_m),
                (value_w, proj_w.at[:, 0:C]),
                (inner_w, proj_w.at[:, C : 2 * C]),
                (outer_w, proj_w.at[:, 2 * C : 3 * C]),
                (mix_w, mixw.at[0:C]),
                (gate_w, gu_w.at[:, 0:F]),
                (up_w, gu_w.at[:, 2 * F : 3 * F]),
                (down_w, dn_w.at[0:F]),
            ]
        )
    ]
    smalls[0].start()
    token_load(0).start()
    smalls[1].start()
    barrier = pltpu.get_barrier_semaphore()
    greet = [to_expert(i) for i in range(half)] + [to_source(i) for i in range(half)]
    greet += [beside(1), beside(-1)]
    greet += [(lax.rem(e + 1, EP), tp), (lax.rem(e + EP - 1, EP), tp)]
    for device in greet:
        pl.semaphore_signal(barrier, inc=1, device_id=device, device_id_type=MESH)
    smalls[2].start()
    for copy in loads[0:4]:
        copy.start()

    def load_tokens(s, carry):
        token_load(s).start()
        return carry

    lax.fori_loop(1, Z, load_tokens, 0)
    for copy in loads[4:] + smalls[3:]:
        copy.start()

    row = lax.broadcasted_iota(jnp.int32, (rows, home), 0)
    tok = lax.broadcasted_iota(jnp.int32, (rows, home), 1)
    expert_of = (2 * (row >> 3) + c).astype(F32)
    slot_of = (row & 3).astype(F32)
    in_block = (tok >> 4) == ((row >> 2) & 1)
    bef_r = lax.broadcasted_iota(jnp.int32, (home, home), 0)
    bef_c = lax.broadcasted_iota(jnp.int32, (home, home), 1)
    before = ((bef_r < bef_c) & ((bef_r >> 4) == (bef_c >> 4))).astype(F32).astype(BF16)
    pick_r = lax.broadcasted_iota(jnp.int32, (tokens, home), 0)
    pick_c = lax.broadcasted_iota(jnp.int32, (tokens, home), 1)
    smalls[0].wait()
    routes_b = routes[...].astype(F32).astype(BF16)

    def routed(zh):
        pick = (pick_r == pick_c + zh * home).astype(F32).astype(BF16)
        named = jnp.dot(routes_b, pick, preferred_element_type=F32)
        h0, h1 = named[0:1, :], named[1:2, :]
        is0, is1 = h0 == expert_of, h1 == expert_of
        rank = jnp.dot((is0 | is1).astype(F32).astype(BF16), before, preferred_element_type=F32)
        at = (rank == slot_of) & in_block
        return h0, h1, at & is0, at & is1

    def dispatch(s):
        y, x = e // SIDE, lax.rem(e, SIDE)
        odd = lax.rem(c + x, 2)
        for dy in (2, 1, 3, 0):
            for n in (0, 1):
                dx = 2 - 2 * n + odd * (4 * n - 1)
                i = (lax.rem(y + dy, SIDE) * SIDE + lax.rem(x + dx, SIDE)) // 2
                remote(send.at[s, i], recv.at[s, slot], disp_send.at[0], disp_recv.at[s], to_expert(i)).start()

    def place(s):
        zh = home_of(s)
        _, _, at0, at1 = routed(zh)
        chosen = (at0 | at1).astype(F32).astype(BF16)
        start = pl.multiple_of(zh * home, home)
        token_load(s).wait()
        rms_rows(raw_e, moe_gain[...], norm_e, start, home)
        for n in range(width // WIDE):
            cols = slice(n * WIDE, (n + 1) * WIDE)
            placed = jnp.dot(chosen, norm_e[pl.ds(start, home), cols], preferred_element_type=F32)
            send[s, :, :, cols] = placed.reshape(half, 2 * CAP, WIDE).astype(BF16)

    swaps = [
        remote(src, dst, swap_send.at[n], swap_recv.at[n], partner)
        for n, (src, dst) in enumerate(
            [
                (gate_w, gu_w.at[:, F : 2 * F]),
                (up_w, gu_w.at[:, 3 * F : 4 * F]),
                (mix_w, mixw.at[C : 2 * C]),
                (down_w, dn_w.at[F : 2 * F]),
            ]
        )
    ]
    halo = remote(halo_out, halo_in, halo_sem.at[0], halo_sem.at[1], (lax.rem(e + 1, EP), tp))
    conv_swap = remote(conv.at[1 - c], conv_all.at[:, C : 2 * C], conv_sem.at[0], conv_sem.at[1], partner)

    def mixer_tail():
        smalls[2].wait()
        loads[0].wait()
        rms_rows(raw_m, mix_gain[...], norm_m, tokens - SHARE, SHARE)
        for n in (1, 2):
            loads[n].wait()
        tail = jnp.dot(norm_m[tokens - SHARE :, :], proj_w[:, 0 : 2 * C], preferred_element_type=F32)
        halo_out[...] = (tail[:, C:] * tail[:, 0:C]).astype(BF16)

    def mixer_proj():
        rms_rows(raw_m, mix_gain[...], norm_m, 0, tokens - SHARE)
        loads[3].wait()
        proj = jnp.dot(norm_m[...], proj_w[...], preferred_element_type=F32)
        gated_in = (proj[:, C : 2 * C] * proj[:, 0:C]).astype(BF16)
        outer_p[...] = proj[:, 2 * C : 3 * C]
        gated[pl.ds(SHARE, tokens), :] = gated_in.astype(F32)

    def mixer_conv():
        halo.wait()
        smalls[3].wait()
        gated[0:SHARE, :] = jnp.where(e > 0, halo_in[...].astype(F32), 0.0)
        mixed = taps[0:1, :] * gated[pl.ds(SHARE - 2, tokens), :]
        mixed = mixed + taps[1:2, :] * gated[pl.ds(SHARE - 1, tokens), :]
        mixed = mixed + taps[2:3, :] * gated[pl.ds(SHARE, tokens), :]
        conv_out = (outer_p[...] * mixed).astype(BF16).reshape(Z, 2, SHARE, C)
        conv[0] = conv_out[:, 0].reshape(Z * SHARE, C)
        conv[1] = conv_out[:, 1].reshape(Z * SHARE, C)
        conv_swap.start()
        swaps[1].start()
        swaps[3].start()
        conv_all[:, 0:C] = conv[c]

    def mix_hop(direction, k, part):
        return remote(
            mix_send.at[direction, k, part],
            mix_recv.at[direction, k, part],
            mixhop_send.at[direction, min(k, 1)],
            mixhop_recv.at[direction, k, part],
            beside(2 * direction - 1),
        )

    def mixer_hop(direction, k):
        zh = lax.rem(z + (2 * direction - 1) * (hops - k) + Z, Z)
        for part in (0, 1):
            total = mix_part[zh, :, part * (width // 2) : (part + 1) * (width // 2)]
            if k > 1 or (k == 1 and direction == 1):
                mix_hop(direction, k - 1, part).wait_recv()
                total = total + mix_recv[direction, k - 1, part].astype(F32)
            mix_send[direction, k, part] = total.astype(BF16)
            mix_hop(direction, k, part).start()

    mix_write = pltpu.make_async_copy(out_v.at[0], out.at[0], out_sem.at[0])

    def mixer_end():
        for direction in (1, 0):
            for part in (0, 1):
                mix_hop(direction, hops - 1, part).wait_recv()
        for part in (0, 1):
            cols = slice(part * (width // 2), (part + 1) * (width // 2))
            total = mix_part[z, :, cols] + mix_recv[1, hops - 1, part].astype(F32)
            out_v[0, :, cols] = (total + mix_recv[0, hops - 1, part].astype(F32)).astype(BF16)
        mix_write.start()

    def mixer_down():
        loads[4].wait()
        swaps[2].wait_recv()
        conv_swap.wait()

        for n in range(width // WIDE):
            cols = slice(n * WIDE, (n + 1) * WIDE)
            part = jnp.dot(conv_all[...], mixw[:, cols], preferred_element_type=F32)
            mix_part[:, :, cols] = part.reshape(Z, SHARE, WIDE)
        mixer_hop(1, 0)
        mixer_hop(0, 1)

    def weigh():
        smalls[4].wait()
        smalls[5].wait()
        h0, h1, at0, at1 = routed(z)
        own_normed = norm_e[pl.ds(pl.multiple_of(z * home, home), home), :]
        contract_last = (((1,), (1,)), ((), ()))
        group_logit = lax.dot_general(router_g[...], own_normed, contract_last, preferred_element_type=F32)
        expert_logit = lax.dot_general(router_e[...], own_normed, contract_last, preferred_element_type=F32)
        group_exp = jnp.exp(group_logit)
        first_of = (lax.broadcasted_iota(jnp.int32, group_exp.shape, 0) * EPG).astype(F32)
        in_group = (h0 >= first_of) & (h0 < first_of + EPG)
        gate = jnp.sum(jnp.where(in_group, group_exp, 0.0), axis=0, keepdims=True) / jnp.sum(
            group_exp, axis=0, keepdims=True
        )
        number = lax.broadcasted_iota(jnp.int32, expert_logit.shape, 0).astype(F32)
        chosen0 = jnp.exp(jnp.sum(jnp.where(number == h0, expert_logit, 0.0), axis=0, keepdims=True))
        chosen1 = jnp.exp(jnp.sum(jnp.where(number == h1, expert_logit, 0.0), axis=0, keepdims=True))
        both = chosen0 + chosen1
        weight = jnp.where(at0, gate * chosen0 / both, 0.0) + jnp.where(at1, gate * chosen1 / both, 0.0)
        weight = weight.T
        high = weight.astype(BF16)
        comb_w[0:home, :] = high
        comb_w[home : 2 * home, :] = (weight - high.astype(F32)).astype(BF16)

    def hop(direction, k, j, h):
        cols = slice(h * fine, (h + 1) * fine)
        return remote(
            rs_send.at[direction, k, j, :, cols],
            rs_recv.at[direction, k, j, :, cols],
            hop_send.at[direction, jnp.minimum(k, 1)],
            hop_recv.at[direction, k, j, h],
            beside(2 * direction - 1),
        )

    def give_back(p, i):
        return remote(ret_send.at[p, i], ret_recv.at[p, slot], back_send.at[0], back_recv.at[p], to_source(i))

    def stage(s, carry):
        for direction, k, when in MIX_HOPS:

            @pl.when(s == when)
            def _():
                mixer_hop(direction, k)

        @pl.when((s > 0) & (s - 1 + AHEAD < Z))
        def _():
            pl.semaphore_wait(credit.at[s - 1], half)
            dispatch(s - 1 + AHEAD)

        @pl.when(s == 0)
        def _():
            for n in (5, 6, 7):
                loads[n].wait()
            for n in (0, 1, 3):
                swaps[n].wait_recv()

        @pl.when(s == Z - 1)
        def _():
            mixer_end()

        @pl.when(s == Z + 1 - AHEAD)
        def _():
            weigh()

        arrived = remote(send.at[s], recv.at[s], disp_send.at[0], disp_recv.at[s], partner)
        arrived.wait_recv()

        @pl.when(s + AHEAD < Z)
        def _():
            for i in range(half):
                pl.semaphore_signal(credit.at[s], inc=1, device_id=to_source(i), device_id_type=MESH)

        x = recv[s].reshape(rows, width)
        gate_up = jnp.dot(x, gu_w[...], preferred_element_type=F32)
        g, u = gate_up[:, 0 : 2 * F], gate_up[:, 2 * F :]
        hidden = (g / (1.0 + jnp.exp(-g)) * u).astype(BF16)
        direction = lax.rem(s, 2)
        k = (s + 1) // 2
        for j in range(PIECES):
            cols = slice(j * piece, (j + 1) * piece)
            side = 1 if j < PIECES // 2 else 0
            acc[...] = jnp.dot(hidden, dn_w[:, cols], preferred_element_type=F32)

            @pl.when(s == 0)
            def _():
                rs_send[side, 0, j] = acc[...].astype(BF16)
                for h in range(FINE):
                    hop(side, 0, j, h).start()

            @pl.when((s > 0) & (s < Z - 1))
            def _():
                @pl.when((k == 1) & (direction == side))
                def _():
                    for h in range(FINE):
                        hop(side, 0, j, h).wait_recv()
                    acc[...] += rs_recv[side, 0, j].astype(F32)

                @pl.when(k > 1)
                def _():
                    for h in range(FINE):
                        hop(direction, k - 1, j, h).wait_recv()
                    acc[...] += rs_recv[direction, k - 1, j].astype(F32)

                rs_send[direction, k, j] = acc[...].astype(BF16)
                for h in range(FINE):
                    hop(direction, k, j, h).start()

            @pl.when(s == Z - 1)
            def _():
                for h in range(FINE):
                    span = slice(h * fine, (h + 1) * fine)
                    for way in (1, 0):
                        hop(way, hops - 1, j, h).wait_recv()
                    total = acc[:, span] + rs_recv[1, hops - 1, j, :, span].astype(F32)
                    total = total + rs_recv[0, hops - 1, j, :, span].astype(F32)
                    p = j * FINE + h
                    ret_send[p] = total.astype(BF16).reshape(half, 2 * CAP, fine)
                    for i in range(half):
                        give_back(p, i).start()

        @pl.when(s + AHEAD < Z)
        def _():
            place(s + AHEAD)

        return carry

    smalls[1].wait()
    place(jnp.int32(0))
    mixer_tail()
    pl.semaphore_wait(barrier, len(greet))
    halo.start()
    dispatch(jnp.int32(0))
    for n in (2, 0):
        swaps[n].start()
    mixer_proj()
    mixer_conv()
    place(jnp.int32(1))
    dispatch(jnp.int32(1))
    mixer_down()

    def place_early(s, carry):
        place(s)
        dispatch(s)
        return carry

    lax.fori_loop(2, AHEAD, place_early, 0)
    lax.fori_loop(0, Z, stage, 0)

    def last(p):
        return remote(comb.at[1 - c, p], comb_in.at[p], last_send.at[0], last_recv.at[p], partner)

    def returned(p):
        return remote(ret_send.at[p], ret_recv.at[p], back_send.at[0], back_recv.at[p], partner)

    def finish(p):
        last(p).wait_recv()
        cols = slice(p * fine, (p + 1) * fine)
        out_v[1, :, cols] = (comb[c, p] + comb_in[p]).astype(BF16)
        write(p).start()

    def write(p):
        cols = slice(p * fine, (p + 1) * fine)
        return pltpu.make_async_copy(out_v.at[1, :, cols], out.at[1, :, cols], out_sem.at[1])

    for p in range(parts):
        returned(p).wait_recv()
        summed = jnp.dot(comb_w[...], ret_recv[p].reshape(rows, fine), preferred_element_type=F32)
        summed = summed[0:home] + summed[home:]
        comb[0, p] = summed[0:SHARE]
        comb[1, p] = summed[SHARE:]
        last(p).start()
        if p > 1:
            finish(p - 2)
    for p in range(parts - 2, parts):
        finish(p)

    for copy in swaps:
        copy.wait_send()
    remote(mix_send.at[1, 0], mix_recv.at[1, 0], mixhop_send.at[1, 0], mixhop_recv.at[1, 0, 0], partner).wait_send()
    remote(send, recv, disp_send.at[0], disp_recv.at[0], partner).wait_send()
    for way in (0, 1):
        later = pl.ds(1, hops - 1)
        near = pl.ds((1 - way) * (PIECES // 2), PIECES // 2)
        remote(
            mix_send.at[way, later], mix_recv.at[way, later], mixhop_send.at[way, 1], mixhop_recv.at[way, 1, 0], partner
        ).wait_send()
        remote(
            rs_send.at[way, 0, near], rs_recv.at[way, 0, near], hop_send.at[way, 0], hop_recv.at[way, 0, 0, 0], partner
        ).wait_send()
        remote(
            rs_send.at[way, later], rs_recv.at[way, later], hop_send.at[way, 1], hop_recv.at[way, 1, 0, 0], partner
        ).wait_send()
    remote(ret_send, ret_recv, back_send.at[0], back_recv.at[0], partner).wait_send()
    remote(comb.at[1 - c], comb_in, last_send.at[0], last_recv.at[0], partner).wait_send()
    pltpu.make_async_copy(out_v.at[1], out.at[1], out_sem.at[1]).wait()
    mix_write.wait()


def solution(mesh):
    EP, TP = mesh.shape["ep"], mesh.shape["tp"]
    Z = TP // 2

    def local(
        mix_tokens,
        mix_gain,
        value_weight,
        inner_weight,
        outer_weight,
        conv_taps,
        mix_weight,
        moe_tokens,
        moe_gain,
        router_group,
        router_expert,
        expert_routes,
        gate_weight,
        up_weight,
        down_weight,
    ):
        tokens, D = mix_tokens.shape
        C = value_weight.shape[1]
        F = gate_weight.shape[2]
        half = EP // 2
        rows = half * 2 * CAP
        piece = D // PIECES
        hops = Z // 2
        fine = piece // FINE
        parts = PIECES * FINE
        hbm = pl.BlockSpec(memory_space=pl.ANY)
        V = pltpu.VMEM
        DMA = pltpu.SemaphoreType.DMA
        both = pl.pallas_call(
            functools.partial(kernel, EP, Z),
            out_shape=jax.ShapeDtypeStruct((2, SHARE, D), BF16),
            in_specs=[hbm] * 15,
            out_specs=hbm,
            scratch_shapes=[
                V((1, D), F32),
                V(conv_taps.shape, F32),
                V((1, D), F32),
                V((router_group.shape[1], D), BF16),
                V((router_expert.shape[1], D), BF16),
                V((2, tokens), jnp.int32),
                V((tokens, D), BF16),
                V((tokens, D), BF16),
                V((tokens, D), BF16),
                V((tokens, D), BF16),
                V((D, 4 * F), BF16),
                V((2 * F, D), BF16),
                V((D, 3 * C), BF16),
                V((2 * C, D), BF16),
                V((Z, half, 2 * CAP, D), BF16),
                V((Z, half, 2 * CAP, D), BF16),
                V((rows, piece), F32),
                V((2, hops, PIECES, rows, piece), BF16),
                V((2, hops, PIECES, rows, piece), BF16),
                V((2, hops, 2, SHARE, D // 2), BF16),
                V((2, hops, 2, SHARE, D // 2), BF16),
                V((SHARE, C), BF16),
                V((SHARE, C), BF16),
                V((SHARE + tokens, C), F32),
                V((tokens, C), F32),
                V((2, Z * SHARE, C), BF16),
                V((Z * SHARE, 2 * C), BF16),
                V((Z, SHARE, D), F32),
                V((4 * SHARE, rows), BF16),
                V((parts, half, 2 * CAP, fine), BF16),
                V((parts, half, 2 * CAP, fine), BF16),
                V((2, parts, SHARE, fine), F32),
                V((parts, SHARE, fine), F32),
                V((2, SHARE, D), BF16),
                DMA((8,)),
                DMA((Z,)),
                DMA((6,)),
                DMA((4,)),
                DMA((4,)),
                DMA((1,)),
                DMA((Z,)),
                pltpu.SemaphoreType.REGULAR((Z,)),
                DMA((2, 2)),
                DMA((2, hops, PIECES, FINE)),
                DMA((2, 2)),
                DMA((2, hops, 2)),
                DMA((2,)),
                DMA((2,)),
                DMA((1,)),
                DMA((parts,)),
                DMA((1,)),
                DMA((parts,)),
                DMA((2,)),
            ],
            compiler_params=pltpu.CompilerParams(
                collective_id=0, has_side_effects=True, vmem_limit_bytes=VMEM_MIB * 1024 * 1024
            ),
            name="mixer_and_experts",
        )(
            mix_tokens,
            mix_gain.reshape(1, D),
            value_weight,
            inner_weight,
            outer_weight,
            conv_taps,
            mix_weight,
            moe_tokens,
            moe_gain.reshape(1, D),
            router_group.T,
            router_expert.T,
            expert_routes.T,
            gate_weight.reshape(D, F),
            up_weight.reshape(D, F),
            down_weight.reshape(F, D),
        )
        return both[0], both[1]

    return jax.shard_map(
        local,
        mesh=mesh,
        in_specs=(
            P("ep", None),
            P(),
            P(None, "tp"),
            P(None, "tp"),
            P(None, "tp"),
            P(None, "tp"),
            P("tp", None),
            P("ep", None),
            P(),
            P(),
            P(),
            P("ep", None),
            P("ep", None, "tp"),
            P("ep", None, "tp"),
            P("ep", "tp", None),
        ),
        out_specs=(P(("ep", "tp"), None), P(("ep", "tp"), None)),
        check_vma=False,
    )
```
